32 devices in a mesh: sp: 4 (over z), fs: 4 (over y, x), tp: 2 (over core).
Axes of the slice: x: 2, y: 2, z: 4, core: 2. Of those that a mesh axis runs over, the one named last changes fastest.
Arguments:
- tokens: bfloat16 [4, 1024, 2048], P('fs', 'sp', 'tp'), may hold values from -6 to 6
- norm_gain: float32 [2048], replicated, may hold values from 0.1 to 1.9
- ret_query: bfloat16 [2048, 1024], P('sp', 'tp'), may hold values from -0.125 to 0.125
- ret_key: bfloat16 [2048, 1024], P('sp', 'tp'), may hold values from -0.125 to 0.125
- ret_value: bfloat16 [2048, 1024], P('sp', 'tp'), may hold values from -0.125 to 0.125
- att_query: bfloat16 [2048, 1024], P('sp', 'tp'), may hold values from -0.125 to 0.125
- att_key: bfloat16 [2048, 256], P('sp', 'tp'), may hold values from -0.125 to 0.125
- att_value: bfloat16 [2048, 256], P('sp', 'tp'), may hold values from -0.125 to 0.125
- log_decay: float32 [4, 4, 1024], P('fs', 'tp', 'sp'), may hold values from -1 to 0
- start_state: float32 [4, 4, 256, 256], P('fs', 'tp'), may hold values from -12 to 12
- ret_gain: float32 [1024], P('tp'), may hold values from 0.1 to 1.9
- sink_logits: float32 [16], P('tp'), may hold values from 1 to 5
- ret_out: bfloat16 [1024, 2048], P('tp', 'fs'), may hold values from -0.1875 to 0.1875
- att_out: bfloat16 [1024, 2048], P('tp', 'fs'), may hold values from -1.5 to 1.5
Outputs:
- mixed: bfloat16 [4, 1024, 2048], P('fs', 'sp', 'tp')
The draws below stay inside these ranges and needn't reach their ends.
All inputs are finite; a program needn't handle non-finite values.
Results may differ from the reference program's by a relative error of at most 0.015.
Values may be sent and summed in bfloat16 or wider, within the bound.
A program may use at most 128 MiB of HBM per device.

```python
import jax
import jax.numpy as jnp
from jax import lax

D = 2048
RETENTION_HEADS = 4
DK = 256
DV = 256
AQH = 16
AKH = 4
HD = 64
WINDOW = 128
BLOCK = 128
TOK_DEV = 256
SEQUENCE_COUNT = 4
SEQUENCE_LENGTH = 1024
N_TP = 2


def draw_log_decay(key, part):
    random_subkeys = jax.random.split(jax.random.fold_in(key, 17), 5)
    blocks = SEQUENCE_LENGTH // TOK_DEV
    ranking = jax.vmap(lambda inner: jax.random.permutation(inner, RETENTION_HEADS))(jax.random.split(random_subkeys[0], SEQUENCE_COUNT))
    fast_heads = (ranking < RETENTION_HEADS // 2).astype(jnp.float32)
    baseline_decay = fast_heads * (3.0 / BLOCK) + (1.0 - fast_heads) * (1.0 / SEQUENCE_LENGTH)
    noise_spread = jax.random.uniform(random_subkeys[1], (SEQUENCE_COUNT, RETENTION_HEADS, blocks), jnp.float32, 0.4, 1.2)
    noise_spread = jnp.repeat(noise_spread, TOK_DEV, axis=-1)
    random_noise = jax.random.uniform(random_subkeys[2], (SEQUENCE_COUNT, RETENTION_HEADS, SEQUENCE_LENGTH), jnp.float32, 0.5, 1.5)
    spike_position = jax.random.randint(random_subkeys[3], (SEQUENCE_COUNT, RETENTION_HEADS, 2), 0, SEQUENCE_LENGTH)
    spike_magnitude = jax.random.uniform(random_subkeys[4], (SEQUENCE_COUNT, RETENTION_HEADS, 2), jnp.float32, 0.2, 0.4)
    position_list = jnp.arange(SEQUENCE_LENGTH, dtype=jnp.int32)
    spike_events = jnp.sum(jnp.where(position_list[None, None, None, :] == spike_position[..., None], jnp.log(1.0 - spike_magnitude)[..., None], 0.0), axis=2)
    return (-baseline_decay[..., None] * noise_spread * random_noise + spike_events).astype(jnp.float32)


def levels(rng, dims, cuts, smallest, high):
    level, own = 1.0, jax.random.fold_in(rng, 6)
    for axis_at, blocks in cuts:
        heights = jnp.exp(jax.random.uniform(jax.random.fold_in(own, axis_at), (blocks,), jnp.float32, smallest / len(cuts), high / len(cuts)))
        level = level * jnp.repeat(heights, dims[axis_at] // blocks).reshape([-1 if axis == axis_at else 1 for axis in range(len(dims))])
    return level


def gaussian(stream_key, dims, deviation, bound, cuts=(), kind=jnp.bfloat16):
    drawn = jax.random.normal(stream_key, dims, jnp.float32) * deviation
    if len(cuts) > 0:
        drawn = levels(stream_key, dims, cuts, -0.22, 0.18) * drawn
    return jnp.clip(drawn, min=-bound, max=bound).astype(kind)


def setup_inputs(seed: int = 0) -> dict:
    key_of = jax.random.split(jax.random.key(seed), 15)
    return {
        "tokens": gaussian(key_of[0], (SEQUENCE_COUNT, SEQUENCE_LENGTH, D), 1.0, 6.0, ((0, 4), (1, 4), (2, 2))),
        "norm_gain": jnp.clip(1.0 + 0.18 * jax.random.normal(key_of[1], (D,), jnp.float32), 0.1, 1.9),
        "ret_query": gaussian(key_of[2], (D, RETENTION_HEADS * DK), D ** -0.5, 0.125, ((0, 4), (1, 2))),
        "ret_key": gaussian(key_of[3], (D, RETENTION_HEADS * DK), D ** -0.5, 0.125, ((0, 4), (1, 2))),
        "ret_value": gaussian(key_of[4], (D, RETENTION_HEADS * DV), D ** -0.5, 0.125, ((0, 4), (1, 2))),
        "att_query": gaussian(key_of[5], (D, AQH * HD), D ** -0.5, 0.125, ((0, 4), (1, 2))),
        "att_key": gaussian(key_of[6], (D, AKH * HD), D ** -0.5, 0.125, ((0, 4), (1, 2))),
        "att_value": gaussian(key_of[7], (D, AKH * HD), D ** -0.5, 0.125, ((0, 4), (1, 2))),
        "log_decay": draw_log_decay(jax.random.fold_in(key_of[14], 71), 0),
        "start_state": gaussian(key_of[9], (SEQUENCE_COUNT, RETENTION_HEADS, DK, DV), (2 * (TOK_DEV // DK) ** 0.5), 12.0, ((0, 4), (1, 2)), jnp.float32),
        "ret_gain": jnp.clip(1.0 + 0.18 * jax.random.normal(key_of[10], (RETENTION_HEADS * DV,), jnp.float32), 0.1, 1.9),
        "sink_logits": jnp.clip(1.0 + 4.0 * jax.random.uniform(key_of[11], (AQH,), jnp.float32) ** levels(key_of[11], (AQH,), ((0, 2),), -0.2, 0.2), 1.0, 5.0),
        "ret_out": gaussian(key_of[12], (RETENTION_HEADS * DV, D), (RETENTION_HEADS * DV) ** -0.5, 0.1875, ((0, 2), (1, 4))),
        "att_out": gaussian(key_of[13], (AQH * HD, D), (AQH * HD // 64) ** -0.5, 1.5, ((0, 2), (1, 4))),
    }


epsilon = 1e-06
exact_result = lax.Precision.HIGHEST

def rotate(values, positions):
    half_dim = values.shape[-1] // 2
    inverse = 1.0 / 10000.0 ** (jnp.arange(half_dim, dtype=jnp.float32) / half_dim)
    angles = positions.astype(jnp.float32)[:, None] * inverse[None, :]
    cosine = jnp.cos(angles)[:, None, :]
    sine_table = jnp.sin(angles)[:, None, :]
    front_half = values[..., :half_dim]
    back_half = values[..., half_dim:]
    return jnp.concatenate([front_half * cosine - back_half * sine_table, front_half * sine_table + back_half * cosine], axis=-1)

def block_step(memory_state, inputs):
    queries, key_matrix_rows, value_matrix_rows, log_rates = inputs
    length_here = log_rates.shape[-1]
    causal = jnp.arange(length_here)[:, None] >= jnp.arange(length_here)[None, :]
    running_totals = jnp.cumsum(log_rates, axis=-1)
    relative = running_totals[:, :, None] - running_totals[:, None, :]
    weight = jnp.where(causal[None], jnp.exp(jnp.where(causal[None], relative, 0.0)), 0.0)
    score_matrix = jnp.einsum('hqd,hkd->hqk', queries, key_matrix_rows, precision=exact_result) * weight
    carried_state = jnp.einsum('hqd,hdv->hqv', queries * jnp.exp(running_totals)[:, :, None], memory_state, precision=exact_result)
    output_rows = jnp.einsum('arf,afu->aru', score_matrix, value_matrix_rows, precision=exact_result) + carried_state
    decay_factors = jnp.exp(running_totals[:, -1:] - running_totals)
    memory_state = memory_state * jnp.exp(running_totals[:, -1])[:, None, None] + jnp.einsum('iwj,iwe->ije', key_matrix_rows * decay_factors[:, :, None], value_matrix_rows, precision=exact_result)
    return (memory_state, output_rows)

def reference(tokens, norm_gain, ret_query, ret_key, ret_value, att_query, att_key, att_value, log_decay, start_state, ret_gain, sink_logits, ret_out, att_out):

    def one_sequence(inputs):
        rows_in, decay_rows, initial = inputs
        as_float = rows_in.astype(jnp.float32)
        normed = (as_float * lax.rsqrt(lax.optimization_barrier(jnp.mean(as_float * as_float, axis=-1, keepdims=True)) + epsilon) * norm_gain).astype(jnp.bfloat16)

        def project(weights):
            return jnp.dot(normed, weights, preferred_element_type=jnp.float32).astype(jnp.bfloat16)
        ret_queries = project(ret_query)
        ret_keys = project(ret_key)
        ret_values = project(ret_value)
        att_queries = project(att_query)
        att_keys = project(att_key)
        att_values = project(att_value)
        positions = jnp.arange(SEQUENCE_LENGTH, dtype=jnp.int32)
        queries = rotate(ret_queries.astype(jnp.float32).reshape(SEQUENCE_LENGTH, RETENTION_HEADS, DK), positions)
        keys_rot = rotate(ret_keys.astype(jnp.float32).reshape(SEQUENCE_LENGTH, RETENTION_HEADS, DK), positions) * DK ** (-0.5)
        values_f = ret_values.astype(jnp.float32).reshape(SEQUENCE_LENGTH, RETENTION_HEADS, DV)
        count = SEQUENCE_LENGTH // BLOCK

        def blocked(array):
            return array.reshape(count, BLOCK, RETENTION_HEADS, array.shape[-1]).transpose(0, 2, 1, 3)
        log_rates = decay_rows.reshape(RETENTION_HEADS, count, BLOCK).transpose(1, 0, 2)
        _, pieces = lax.scan(block_step, initial, (blocked(queries), blocked(keys_rot), blocked(values_f), log_rates))
        retained = pieces.transpose(0, 2, 1, 3).reshape(SEQUENCE_LENGTH, RETENTION_HEADS, DV)
        centred = retained - lax.optimization_barrier(jnp.mean(retained, axis=-1, keepdims=True))
        variance = lax.optimization_barrier(jnp.mean(centred * centred, axis=-1, keepdims=True))
        ret_hidden = ((centred * lax.rsqrt(variance + epsilon)).reshape(SEQUENCE_LENGTH, RETENTION_HEADS * DV) * ret_gain).astype(jnp.bfloat16)
        windows = SEQUENCE_LENGTH // WINDOW
        groups = AQH // AKH
        grouped_q = att_queries.reshape(windows, WINDOW, AKH, groups, HD).astype(jnp.float32)

        def banded(array):
            blocks_now = array.reshape(windows, WINDOW, AKH, HD)
            earlier = jnp.concatenate([jnp.zeros((1, WINDOW, AKH, HD), array.dtype), blocks_now[:-1]], axis=0)
            return jnp.concatenate([earlier, blocks_now], axis=1).astype(jnp.float32)
        key_band = banded(att_keys)
        value_band = banded(att_values)
        score_matrix = jnp.einsum('nqhgd,nkhd->nhgqk', grouped_q, key_band) * HD ** (-0.5)
        query_index = WINDOW + jnp.arange(WINDOW)
        key_index = jnp.arange(2 * WINDOW)
        allowed = (key_index[None, :] <= query_index[:, None]) & (query_index[:, None] - key_index[None, :] < WINDOW)
        present = (jnp.arange(windows)[:, None] > 0) | (key_index >= WINDOW)[None, :]
        visible = (allowed[None] & present[:, None, :])[:, None, None]
        expo = jnp.exp(jnp.where(visible, score_matrix, -1e+30))
        summed = lax.optimization_barrier(jnp.sum(expo, axis=-1, keepdims=True)) + jnp.exp(sink_logits).reshape(1, AKH, groups, 1, 1)
        probs = (expo / summed).astype(jnp.bfloat16)
        att_hidden = jnp.einsum('nhgqk,nkhd->nqhgd', probs.astype(jnp.float32), value_band).astype(jnp.bfloat16).reshape(SEQUENCE_LENGTH, AQH * HD)
        ret_cols = RETENTION_HEADS * DV // N_TP
        att_cols = AQH * HD // N_TP
        mixed = jnp.zeros((SEQUENCE_LENGTH, D), jnp.float32)
        for group_index in range(N_TP):
            partial_value = jnp.dot(ret_hidden[:, group_index * ret_cols:(group_index + 1) * ret_cols], ret_out[group_index * ret_cols:(group_index + 1) * ret_cols], preferred_element_type=jnp.float32)
            partial_value = partial_value + jnp.dot(att_hidden[:, group_index * att_cols:(group_index + 1) * att_cols], att_out[group_index * att_cols:(group_index + 1) * att_cols], preferred_element_type=jnp.float32)
            rounded = lax.optimization_barrier(partial_value.astype(jnp.bfloat16))
            mixed = mixed + rounded.astype(jnp.float32)
        return mixed.astype(jnp.bfloat16)
    return lax.map(one_sequence, (tokens, log_decay, start_state))
```

```python
import functools

import jax
import jax.numpy as jnp
import numpy as np
from jax import lax
from jax.experimental import pallas as pl
from jax.experimental.pallas import tpu as pltpu
from jax.sharding import PartitionSpec as P

DK = 256
DV = 256
HD = 64
WINDOW = 128
BLOCK = 128


epsilon = 1e-06
exact_result = lax.Precision.HIGHEST


def carried_in(array, axis, combine, identity):
    peers, mine = (lax.axis_size(axis), lax.axis_index(axis))
    everything = jax.tree.map(
        lambda part, kind: lax.all_gather(part.astype(kind), axis),
        array,
        (jnp.bfloat16, jnp.bfloat16),
    )
    start = jax.tree.map(
        lambda part, zero: jnp.broadcast_to(jnp.asarray(zero, part.dtype), part.shape),
        array,
        identity,
    )

    def hop(k, before):
        reached = k < mine
        new = combine(
            before, jax.tree.map(lambda part, own: part[k].astype(own.dtype), everything, array)
        )
        return jax.tree.map(lambda a, b: jnp.where(reached, a, b), new, before)

    return lax.fori_loop(0, peers, hop, start)


def passed_along(block, axis, distance):
    devices = range(lax.axis_size(axis))
    route = [(i - distance, i) for i in devices if i - distance in devices]
    return lax.ppermute(block, axis, route)


def rotate(values, positions):
    half_dim = values.shape[-1] // 2
    inverse = 1.0 / 10000.0 ** (jnp.arange(half_dim, dtype=jnp.float32) / half_dim)
    angles = positions.astype(jnp.float32)[:, None] * inverse[None, :]
    cosine = jnp.cos(angles)[:, None, :]
    sine_table = jnp.sin(angles)[:, None, :]
    front_half = values[..., :half_dim]
    back_half = values[..., half_dim:]
    return jnp.concatenate(
        [
            front_half * cosine - back_half * sine_table,
            front_half * sine_table + back_half * cosine,
        ],
        axis=-1,
    )


def block_step(memory_state, inputs):
    queries, key_matrix_rows, value_matrix_rows, log_rates = inputs
    length_here = log_rates.shape[-1]
    causal = jnp.arange(length_here)[:, None] >= jnp.arange(length_here)[None, :]
    running_totals = jnp.cumsum(log_rates, axis=-1)
    relative = running_totals[:, :, None] - running_totals[:, None, :]
    weight = jnp.where(causal[None], jnp.exp(jnp.where(causal[None], relative, 0.0)), 0.0)
    score_matrix = (
        jnp.einsum("hqd,hkd->hqk", queries, key_matrix_rows, precision=exact_result) * weight
    )
    carried_state = jnp.einsum(
        "hqd,hdv->hqv",
        queries * jnp.exp(running_totals)[:, :, None],
        memory_state,
        precision=exact_result,
    )
    output_rows = (
        jnp.einsum("arf,afu->aru", score_matrix, value_matrix_rows, precision=exact_result)
        + carried_state
    )
    decay_factors = jnp.exp(running_totals[:, -1:] - running_totals)
    memory_state = memory_state * jnp.exp(running_totals[:, -1])[:, None, None] + jnp.einsum(
        "iwj,iwe->ije",
        key_matrix_rows * decay_factors[:, :, None],
        value_matrix_rows,
        precision=exact_result,
    )
    return (memory_state, output_rows)


def chain(earlier, later):
    return (earlier[0] * later[0], earlier[1] * later[0][:, None, None] + later[1])


def shards(
    tokens,
    norm_gain,
    ret_query,
    ret_key,
    ret_value,
    att_query,
    att_key,
    att_value,
    log_decay,
    start_state,
    ret_gain,
    sink_logits,
    ret_out,
    att_out,
):
    gathered = lax.all_gather(tokens[0], "tp", axis=1, tiled=True)
    row_count = gathered.shape[0]
    as_float = gathered.astype(jnp.float32)
    normed = (
        as_float
        * lax.rsqrt(jnp.mean(as_float * as_float, axis=-1, keepdims=True) + epsilon)
        * norm_gain
    ).astype(jnp.bfloat16)
    offset = lax.axis_index("sp") * row_count
    positions = offset + jnp.arange(row_count, dtype=jnp.int32)
    weights = (ret_query, ret_key, ret_value, att_query, att_key, att_value)
    pieces = (
        lax.all_gather(weights[0], "sp", axis=0, tiled=True),
        lax.all_gather(weights[1], "sp", axis=0, tiled=True),
        lax.all_gather(weights[2], "sp", axis=0, tiled=True),
        lax.all_gather(weights[3], "sp", axis=0, tiled=True),
        lax.all_gather(weights[4], "sp", axis=0, tiled=True),
        lax.all_gather(weights[5], "sp", axis=0, tiled=True),
    )
    projected = tuple(
        (jnp.dot(normed, piece, preferred_element_type=jnp.float32) for piece in pieces)
    )
    rounded = tuple((product_f.astype(jnp.bfloat16) for product_f in projected))
    projected = rounded[:3]
    head_count = projected[0].shape[1] // DK
    queries = rotate(projected[0].astype(jnp.float32).reshape(row_count, head_count, DK), positions)
    keys_rot = rotate(
        projected[1].astype(jnp.float32).reshape(row_count, head_count, DK), positions
    ) * DK ** (-0.5)
    values_f = projected[2].astype(jnp.float32).reshape(row_count, head_count, DV)
    log_rates = log_decay[0]
    count = row_count // BLOCK

    def blocked(array):
        return array.reshape(count, BLOCK, head_count, array.shape[-1]).transpose(0, 2, 1, 3)

    rates_blocked = log_rates.reshape(head_count, count, BLOCK).transpose(1, 0, 2)
    local_state, pieces = lax.scan(
        block_step,
        jnp.zeros((head_count, DK, DV), jnp.float32),
        (blocked(queries), blocked(keys_rot), blocked(values_f), rates_blocked),
    )
    local_out = pieces.transpose(0, 2, 1, 3).reshape(row_count, head_count, DV)
    running_totals = jnp.cumsum(log_rates, axis=-1)
    device_decay = jnp.exp(running_totals[:, -1])
    identity = (jnp.ones((head_count,), jnp.float32), jnp.zeros((head_count, DK, DV), jnp.float32))
    prior_decay, prior_state = carried_in((device_decay, local_state), "sp", chain, identity)
    incoming = prior_state + prior_decay[:, None, None] * start_state[0]
    retained = local_out + jnp.einsum(
        "thd,hdv->thv",
        queries * jnp.exp(running_totals).T[:, :, None],
        incoming,
        precision=exact_result,
    )
    centred = retained - jnp.mean(retained, axis=-1, keepdims=True)
    variance = jnp.mean(centred * centred, axis=-1, keepdims=True)
    ret_hidden = (
        (centred * lax.rsqrt(variance + epsilon)).reshape(row_count, head_count * DV) * ret_gain
    ).astype(jnp.bfloat16)
    att_queries, att_keys, att_values = rounded[3:]
    kv_heads = att_keys.shape[1] // HD
    groups = att_queries.shape[1] // HD // kv_heads
    earlier_keys, earlier_values = passed_along(
        (att_keys[row_count - WINDOW :], att_values[row_count - WINDOW :]), "sp", 1
    )
    extended_keys = jnp.concatenate([earlier_keys, att_keys], axis=0)
    extended_values = jnp.concatenate([earlier_values, att_values], axis=0)
    windows = row_count // WINDOW

    def banded(array):
        earlier = array[:row_count].reshape(windows, WINDOW, kv_heads, HD)
        current = array[WINDOW:].reshape(windows, WINDOW, kv_heads, HD)
        return jnp.concatenate([earlier, current], axis=1)

    key_band = banded(extended_keys)
    value_band = banded(extended_values)
    grouped_q = att_queries.reshape(windows, WINDOW, kv_heads, groups, HD)
    score_matrix = jnp.einsum(
        "nqhgd,nkhd->nhgqk", grouped_q, key_band, preferred_element_type=jnp.float32
    ) * HD ** (-0.5)
    query_index = WINDOW + jnp.arange(WINDOW)
    key_index = jnp.arange(2 * WINDOW)
    allowed = (key_index[None, :] <= query_index[:, None]) & (
        query_index[:, None] - key_index[None, :] < WINDOW
    )
    key_place = offset - WINDOW + jnp.arange(windows)[:, None] * WINDOW + key_index[None, :]
    visible = (allowed[None] & (key_place >= 0)[:, None, :])[:, None, None]
    expo = jnp.exp(jnp.where(visible, score_matrix, -1e30))
    summed = jnp.sum(expo, axis=-1, keepdims=True) + jnp.exp(sink_logits).reshape(
        1, kv_heads, groups, 1, 1
    )
    probs = (expo / summed).astype(jnp.bfloat16)
    attended = jnp.einsum(
        "nhgqk,nkhd->nqhgd", probs, value_band, preferred_element_type=jnp.float32
    )
    att_hidden = attended.astype(jnp.bfloat16).reshape(row_count, kv_heads * groups * HD)
    ret_width = ret_hidden.shape[1]
    joined = jnp.concatenate([ret_hidden, att_hidden], axis=1)[None]
    piece = lax.all_gather(joined, "fs", axis=0, tiled=True)
    product = jnp.einsum(
        "srh,hd->srd", piece[:, :, :ret_width], ret_out, preferred_element_type=jnp.float32
    )
    product = product + jnp.einsum(
        "srh,hd->srd", piece[:, :, ret_width:], att_out, preferred_element_type=jnp.float32
    )
    partial_rows = product.astype(jnp.bfloat16)
    regrouped = lax.all_to_all(partial_rows, "fs", split_axis=0, concat_axis=2, tiled=True)
    mixed = lax.psum_scatter(
        regrouped[0].astype(jnp.float32).astype(jnp.bfloat16), "tp", scatter_dimension=1, tiled=True
    )
    return mixed[None]


MESH = pl.DeviceIdType.MESH
F32 = jnp.float32
BF16 = jnp.bfloat16
GAIN_ROW = 0
DECAY_ROW = 1
SINK_ROW = 8


def dot(a, b):
    return jnp.dot(a, b, preferred_element_type=F32)


def dot_t(a, b):
    return lax.dot_general(a, b, (((1,), (1,)), ((), ())), preferred_element_type=F32)


def dot_l(a, b):
    return lax.dot_general(a, b, (((0,), (0,)), ((), ())), preferred_element_type=F32)


def fused(
    n_sp, n_fs, tok, ngain, rq, rk, rv, aq, ak, av, small, start, ro, ao, cos, sin, out,
    toks, ss_mine, ss_peer, w, wo, sm, s0, proj, kv, hid, hin, state,
    send, wsem, wpsem, smsem, ssem, sssem, tsem, osem, hsem, lsem,
):
    z, f, c = lax.axis_index("sp"), lax.axis_index("fs"), lax.axis_index("tp")
    peer = 1 - c
    rows, half = tok.shape
    depth = rq.shape[0]
    quarter = depth // n_fs
    heads_core = rq.shape[1] // DK
    kvw = ak.shape[1]
    groups = aq.shape[1] // kvw
    qw = groups * HD
    ret_cols, att_cols = 3 * DK, qw + 2 * kvw
    sub = lax.rem(z, heads_core)
    is0, is1 = c == 0, c == 1

    barrier = pltpu.get_barrier_semaphore()
    count = 0

    def greet(**where):
        pl.semaphore_signal(barrier, inc=1, device_id=where, device_id_type=MESH)

    greet(tp=peer)
    for t in range(2):
        for i in range(1, n_sp):
            greet(sp=lax.rem(z + i, n_sp), tp=jnp.int32(t))
            count += 1
        for i in range(1, n_fs):
            greet(fs=lax.rem(f + i, n_fs), tp=jnp.int32(t))
            count += 1
    pl.semaphore_wait(barrier, count + 1)

    sent = []
    slots = iter(range(send.shape[0]))

    def both(a, b):
        if a is None:
            return b
        return a if b is None else jnp.logical_and(a, b)

    def remote(cond, src, dst, rsem, slot=None, **where):
        slot = next(slots) if slot is None else slot
        copy = pltpu.make_async_remote_copy(
            src_ref=src, dst_ref=dst, send_sem=send.at[slot], recv_sem=rsem,
            device_id=where, device_id_type=MESH,
        )
        sent.append((cond, copy))
        if cond is None:
            copy.start()
        else:
            pl.when(cond)(copy.start)

    def local(cond, src, dst, sem):
        pl.when(cond)(pltpu.make_async_copy(src, dst, sem).start)

    def arrived(dst, sem):
        pltpu.make_async_copy(dst, dst, sem).wait()

    def wrows(at, n):
        return pl.ds(pl.multiple_of(at, quarter), n)

    def pieces(j, kind):
        if kind == 0:
            return [(a, pl.ds(j * DK, DK), pl.ds(i * DK, DK)) for i, a in enumerate((rq, rk, rv))]
        return [
            (aq, pl.ds(j * qw, qw), pl.ds(0, qw)),
            (ak, pl.ds(0, kvw), pl.ds(qw, kvw)),
            (av, pl.ds(0, kvw), pl.ds(qw + kvw, kvw)),
        ]

    mine = pl.ds(pl.multiple_of(f * quarter, quarter), quarter)
    for j in range(heads_core):
        p = heads_core * c + j
        away = p != z
        here = p == z
        for kind in range(2):
            remote(away, small, sm.at[z], smsem.at[z], sp=p, tp=jnp.int32(kind))
            for i, (a, cs, cd) in enumerate(pieces(j, kind)):
                remote(
                    away, a.at[mine, cs], w.at[wrows(z * depth + f * quarter, quarter), cd],
                    wsem.at[z, i], sp=p, tp=jnp.int32(kind),
                )
        remote(here, small, sm.at[z], smsem.at[z], tp=peer)
        local(here, small, sm.at[z], smsem.at[z])
        for kind in range(2):
            same, other = both(here, c == kind), both(here, c != kind)
            for i, (a, cs, cd) in enumerate(pieces(j, kind)):
                dst = w.at[wrows(z * depth, depth), cd]
                local(same, a.at[:, cs], dst, wsem.at[z, i])
                remote(other, a.at[:, cs], dst, wsem.at[z, i], tp=peer)
        local(both(here, is0), start.at[j], s0, ssem)
        remote(both(here, is1), start.at[j], s0, ssem, tp=peer)

    x = tok[...].astype(F32)
    sq = x * x
    part = sq[:, :128]
    for i in range(1, half // 128):
        part = part + sq[:, i * 128 : (i + 1) * 128]
    ss_mine[...] = part
    remote(None, ss_mine, ss_peer, sssem, tp=peer)
    arrived(ss_peer, sssem)
    mean = jnp.sum(ss_mine[...] + ss_peer[...], axis=-1, keepdims=True) / (2 * half)
    scale = lax.rsqrt(mean + epsilon)
    g = ngain[:, pl.ds(pl.multiple_of(c * half, 128), half)]
    toks[z, c] = (tok[...].astype(F32) * scale * g).astype(BF16)

    def spread(zs, cond, up, down):
        block = toks.at[zs, c]
        if up is not None:
            remote(both(cond, up), block, block, tsem.at[zs, c], sp=lax.rem(z + 1, n_sp))
        if down is not None:
            remote(both(cond, down), block, block, tsem.at[zs, c], sp=lax.rem(z + n_sp - 1, n_sp))
        remote(cond, block, block, tsem.at[zs, c], tp=peer)

    spread(z, None, z < n_sp - 1, z > 0)

    def widths(act):
        for kind, cols in ((0, ret_cols), (1, att_cols)):
            act(c == kind, pl.ds(0, cols))

    for i in range(1, n_sp):
        zs = lax.rem(z + i, n_sp)
        at = wrows(zs * depth + f * quarter, quarter)
        for kind in range(2):
            @pl.when(c == kind)
            def _():
                for n, (_, _, cd) in enumerate(pieces(0, kind)):
                    arrived(w.at[at, cd], wsem.at[zs, n])
        base = [next(slots) for _ in range(n_fs - 1)]
        for kind, cols in ((0, ret_cols), (1, att_cols)):
            for k in range(1, n_fs):
                block = w.at[at, pl.ds(0, cols)]
                remote(c == kind, block, block, wpsem.at[zs, f], slot=base[k - 1],
                       fs=lax.rem(f + k, n_fs))

    fs_core = n_fs // 2
    owner = f // fs_core
    jf = lax.rem(f, fs_core)
    out_rows, out_cols = ro.shape
    for kind, a in enumerate((ro, ao)):
        dst = wo.at[kind, pl.ds(pl.multiple_of(c * out_rows, out_rows), out_rows),
                    pl.ds(pl.multiple_of(jf * out_cols, out_cols), out_cols)]
        sem = osem.at[kind, c, jf]
        for k in range(1, n_fs):
            remote(None, a, dst, sem, fs=lax.rem(f + k, n_fs), tp=owner)
        local(c == owner, a, dst, sem)
        remote(c != owner, a, dst, sem, tp=peer)

    for kind, cols in ((0, ret_cols), (1, att_cols)):
        @pl.when(c == kind)
        def _():
            for n, (_, _, cd) in enumerate(pieces(0, kind)):
                arrived(w.at[wrows(z * depth, depth), cd], wsem.at[z, n])
            for i in range(1, n_sp):
                zs = lax.rem(z + i, n_sp)
                for k in range(1, n_fs):
                    fs = lax.rem(f + k, n_fs)
                    arrived(w.at[wrows(zs * depth + fs * quarter, quarter), pl.ds(0, cols)],
                            wpsem.at[zs, fs])
    for i in range(n_sp):
        arrived(sm.at[i], smsem.at[i])
    kv[pl.ds(0, WINDOW), :] = jnp.zeros((WINDOW, kv.shape[1]), BF16)

    def project(zs):
        at = pl.ds(pl.multiple_of(zs * rows, rows), rows)

        def tile(cols):
            return dot(toks[zs, 0], w[pl.ds(0, half), cols]) + dot(toks[zs, 1], w[pl.ds(half, half), cols])

        @pl.when(is0)
        def _():
            @pl.loop(0, 3)
            def _(i):
                cols = pl.ds(pl.multiple_of(i * DK, DK), DK)
                proj[at, cols] = tile(cols).astype(BF16)

            co, si = cos[at, :], sin[at, :]
            h = DK // 2
            for i, factor in ((0, 1.0), (1, DK ** (-0.5))):
                a = proj[at, pl.ds(i * DK, h)].astype(F32)
                b = proj[at, pl.ds(i * DK + h, h)].astype(F32)
                proj[at, pl.ds(i * DK, h)] = ((a * co - b * si) * factor).astype(BF16)
                proj[at, pl.ds(i * DK + h, h)] = ((a * si + b * co) * factor).astype(BF16)

        @pl.when(is1)
        def _():
            proj[at, pl.ds(0, qw)] = tile(pl.ds(0, qw)).astype(BF16)
            both_kv = tile(pl.ds(qw, 2 * kvw))
            to = pl.ds(pl.multiple_of(WINDOW + zs * rows, WINDOW), rows)
            for n in range(2):
                got = both_kv[:, n * kvw : n * kvw + HD]
                for s in range(1, heads_core):
                    got = jnp.where(sub == s, both_kv[:, n * kvw + s * HD : n * kvw + (s + 1) * HD], got)
                kv[to, pl.ds(n * 128, HD)] = got.astype(BF16)

    def peer_half(zs):
        arrived(toks.at[zs, peer], tsem.at[zs, peer])

    def later(zs, cond):
        def run():
            peer_half(zs)
            project(zs)
        if cond is None:
            run()
        else:
            pl.when(cond)(run)

    waiting = [(z, None)]
    for d in range(1, n_sp):
        new = []
        for s in (-1, 1):
            zs = z + s * d
            ok = zs >= 0 if s < 0 else zs < n_sp
            zs = jnp.clip(zs, 0, n_sp - 1)
            pl.when(ok)(functools.partial(arrived, toks.at[zs, c], tsem.at[zs, c]))
            if s < 0:
                spread(zs, ok, z < n_sp - 1, None)
            else:
                spread(zs, ok, None, z > 0)
            new.append((zs, ok))
            if waiting:
                later(*waiting.pop(0))
        for item in waiting:
            later(*item)
        waiting = new
    for item in waiting:
        later(*item)

    lane = lax.broadcasted_iota(jnp.int32, (BLOCK, BLOCK), 1)
    row = lax.broadcasted_iota(jnp.int32, (BLOCK, BLOCK), 0)
    per = rows // BLOCK

    def retention(p, i):
        b = p * per + i
        at = pl.ds(pl.multiple_of(b * BLOCK, BLOCK), BLOCK)
        l = sm[p, pl.ds(DECAY_ROW, 1), pl.ds(pl.multiple_of(sub * rows + i * BLOCK, BLOCK), BLOCK)]
        cum = jnp.sum(jnp.where(lane <= row, l, 0.0), axis=1, keepdims=True)
        cum_row = jnp.sum(jnp.where(lane == row, cum, 0.0), axis=0, keepdims=True)
        total = jnp.sum(l, axis=1, keepdims=True)
        weight = jnp.where(lane <= row, jnp.exp(jnp.where(lane <= row, cum - cum_row, 0.0)), 0.0)
        q, k, v = (proj[at, pl.ds(n * DK, DK)] for n in range(3))
        st = state[...]
        scores = (dot_t(q, k) * weight).astype(BF16)
        o = dot(scores, v) + dot((q.astype(F32) * jnp.exp(cum)).astype(BF16), st.astype(BF16))
        kd = (k.astype(F32) * jnp.exp(total - cum)).astype(BF16)
        state[...] = st * jnp.exp(total) + dot_l(kd, v)
        centred = o - jnp.mean(o, axis=-1, keepdims=True)
        var = jnp.mean(centred * centred, axis=-1, keepdims=True)
        gain = sm[z, pl.ds(GAIN_ROW, 1), pl.ds(pl.multiple_of(sub * DV, DV), DV)]
        hid[at, :] = (centred * lax.rsqrt(var + epsilon) * gain).astype(BF16)

    lane2 = lax.broadcasted_iota(jnp.int32, (WINDOW, 2 * WINDOW), 1)
    row2 = lax.broadcasted_iota(jnp.int32, (WINDOW, 2 * WINDOW), 0)

    def attention(p, i):
        b = p * per + i
        at = pl.ds(pl.multiple_of(b * WINDOW, WINDOW), WINDOW)
        band = pl.ds(pl.multiple_of(b * WINDOW, WINDOW), 2 * WINDOW)
        k, v = kv[band, pl.ds(0, HD)], kv[band, pl.ds(128, HD)]
        visible = (lane2 <= row2 + WINDOW) & (lane2 > row2) & (lane2 + b * WINDOW >= WINDOW)
        sinks = sm[z, pl.ds(SINK_ROW, heads_core * groups), pl.ds(0, 128)]
        res = []
        for h in range(groups):
            q = proj[at, pl.ds(h * HD, HD)]
            score = dot_t(q, k) * HD ** (-0.5)
            e = jnp.exp(jnp.where(visible, score, -1e30))
            logit = sinks[h : h + 1, :1]
            for s in range(1, heads_core):
                logit = jnp.where(sub == s, sinks[s * groups + h : s * groups + h + 1, :1], logit)
            sink = jnp.exp(logit)
            total = jnp.sum(e, axis=-1, keepdims=True) + sink
            res.append(dot((e / total).astype(BF16), v))
        hid[at, :] = jnp.concatenate(res, axis=1).astype(BF16)

    @pl.when(is0)
    def _():
        arrived(s0, ssem)
        state[...] = s0[...]

    for p in range(n_sp):
        @pl.when(is0)
        def _():
            pl.loop(0, per)(functools.partial(retention, p))

        @pl.when(is1)
        def _():
            pl.loop(0, per)(functools.partial(attention, p))

        block = hid.at[pl.ds(p * rows, rows)]
        remote(z != p, block, hin.at[c, z], hsem.at[c, z], sp=jnp.int32(p))
        local(z == p, block, hin.at[c, z], hsem.at[c, z])

    for i in range(n_sp):
        zs = lax.rem(z + i, n_sp)
        arrived(hin.at[c, zs], hsem.at[c, zs])
        remote(None, hin.at[c, zs], hin.at[c, zs], hsem.at[c, zs], tp=peer)
    for kind in range(2):
        for cs in range(2):
            for j in range(fs_core):
                arrived(wo.at[kind, pl.ds(cs * out_rows, out_rows), pl.ds(j * out_cols, out_cols)],
                        osem.at[kind, cs, j])
    for zs in range(n_sp):
        arrived(hin.at[peer, zs], hsem.at[peer, zs])

    @pl.loop(0, out.shape[1] // 256)
    def _(i):
        cols = pl.ds(pl.multiple_of(i * 256, 256), 256)
        acc = None
        for kind in range(2):
            for h in range(n_sp):
                width = hin.shape[3]
                term = dot(hin[kind, h], wo[kind, pl.ds(h * width, width), cols])
                acc = term if acc is None else acc + term
        out[:, cols] = acc.astype(BF16)

    for cond, copy in sent:
        if cond is None:
            copy.wait_send()
        else:
            pl.when(cond)(copy.wait_send)


def layer(mesh, *args):
    (tokens, norm_gain, ret_query, ret_key, ret_value, att_query, att_key, att_value,
     log_decay, start_state, ret_gain, sink_logits, ret_out, att_out) = args
    n_sp, n_fs, n_tp = mesh.shape["sp"], mesh.shape["fs"], mesh.shape["tp"]
    heads = ret_query.shape[1] // DK
    kv_heads = att_key.shape[1] // HD
    rows, half = tokens.shape[1:]
    whole_heads = (
        n_tp == 2 and n_fs % 2 == 0 and heads * n_tp == n_sp and kv_heads == heads
        and att_query.shape[1] == ret_query.shape[1]
    )
    if not whole_heads:
        return shards(*args)
    depth = ret_query.shape[0]
    wide = heads * rows
    decay = log_decay[0].reshape(1, wide)
    small = jnp.concatenate([
        jnp.pad(ret_gain[None], ((0, 0), (0, wide - ret_gain.shape[0]))),
        decay,
        jnp.zeros((SINK_ROW - 2, wide), F32),
        jnp.broadcast_to(sink_logits[:, None], (sink_logits.shape[0], wide)),
    ])
    h = DK // 2
    inverse = np.float32(1.0) / np.float32(10000.0) ** (np.arange(h, dtype=np.float32) / np.float32(h))
    angles = np.arange(n_sp * rows, dtype=np.float32)[:, None] * inverse[None, :]
    cos = jnp.asarray(np.cos(angles), F32)
    sin = jnp.asarray(np.sin(angles), F32)
    length = n_sp * rows
    vm = pl.BlockSpec(memory_space=pltpu.VMEM)
    hbm = pl.BlockSpec(memory_space=pl.ANY)
    dma = pltpu.SemaphoreType.DMA
    res = pl.pallas_call(
        functools.partial(fused, n_sp, n_fs),
        out_shape=jax.ShapeDtypeStruct((rows, half), BF16),
        in_specs=[vm, vm] + [hbm] * 6 + [vm, hbm, hbm, hbm, vm, vm],
        out_specs=vm,
        scratch_shapes=[
            pltpu.VMEM((n_sp, 2, rows, half), BF16),
            pltpu.VMEM((rows, 128), F32),
            pltpu.VMEM((rows, 128), F32),
            pltpu.VMEM((n_sp * depth, 3 * DK), BF16),
            pltpu.VMEM((2, 2 * ret_out.shape[0], n_fs // 2 * ret_out.shape[1]), BF16),
            pltpu.VMEM((n_sp,) + small.shape, F32),
            pltpu.VMEM((DK, DV), F32),
            pltpu.VMEM((length, 3 * DK), BF16),
            pltpu.VMEM((WINDOW + length, 256), BF16),
            pltpu.VMEM((length, DV), BF16),
            pltpu.VMEM((2, n_sp, rows, DV), BF16),
            pltpu.VMEM((DK, DV), F32),
            dma((100,)),
            dma((n_sp, 3)),
            dma((n_sp, n_fs)),
            dma((n_sp,)),
            dma,
            dma,
            dma((n_sp, 2)),
            dma((2, 2, n_fs // 2)),
            dma((2, n_sp)),
            dma,
        ],
        compiler_params=pltpu.CompilerParams(
            collective_id=0, has_side_effects=True, vmem_limit_bytes=48 * 1024 * 1024
        ),
    )(
        tokens[0], norm_gain[None], ret_query, ret_key, ret_value, att_query, att_key, att_value,
        small, start_state[0], ret_out, att_out, cos, sin,
    )
    return res[None]


def solution(mesh):
    placed = (
        P("fs", "sp", "tp"),
        P(),
        P("sp", "tp"),
        P("sp", "tp"),
        P("sp", "tp"),
        P("sp", "tp"),
        P("sp", "tp"),
        P("sp", "tp"),
        P("fs", "tp", "sp"),
        P("fs", "tp", None, None),
        P("tp"),
        P("tp"),
        P("tp", "fs"),
        P("tp", "fs"),
    )
    return jax.shard_map(
        functools.partial(layer, mesh), mesh=mesh, in_specs=placed, out_specs=P("fs", "sp", "tp"), check_vma=False
    )
```

```python
import functools

import jax
import jax.numpy as jnp
import numpy as np
from jax import lax
from jax.experimental import pallas as pl
from jax.experimental.pallas import tpu as pltpu
from jax.sharding import PartitionSpec as P

DK = 256
DV = 256
HD = 64
WINDOW = 128
BLOCK = 128


epsilon = 1e-06
exact_result = lax.Precision.HIGHEST


def carried_in(array, axis, combine, identity):
    peers, mine = (lax.axis_size(axis), lax.axis_index(axis))
    everything = jax.tree.map(
        lambda part, kind: lax.all_gather(part.astype(kind), axis),
        array,
        (jnp.bfloat16, jnp.bfloat16),
    )
    start = jax.tree.map(
        lambda part, zero: jnp.broadcast_to(jnp.asarray(zero, part.dtype), part.shape),
        array,
        identity,
    )

    def hop(k, before):
        reached = k < mine
        new = combine(
            before, jax.tree.map(lambda part, own: part[k].astype(own.dtype), everything, array)
        )
        return jax.tree.map(lambda a, b: jnp.where(reached, a, b), new, before)

    return lax.fori_loop(0, peers, hop, start)


def passed_along(block, axis, distance):
    devices = range(lax.axis_size(axis))
    route = [(i - distance, i) for i in devices if i - distance in devices]
    return lax.ppermute(block, axis, route)


def rotate(values, positions):
    half_dim = values.shape[-1] // 2
    inverse = 1.0 / 10000.0 ** (jnp.arange(half_dim, dtype=jnp.float32) / half_dim)
    angles = positions.astype(jnp.float32)[:, None] * inverse[None, :]
    cosine = jnp.cos(angles)[:, None, :]
    sine_table = jnp.sin(angles)[:, None, :]
    front_half = values[..., :half_dim]
    back_half = values[..., half_dim:]
    return jnp.concatenate(
        [
            front_half * cosine - back_half * sine_table,
            front_half * sine_table + back_half * cosine,
        ],
        axis=-1,
    )


def block_step(memory_state, inputs):
    queries, key_matrix_rows, value_matrix_rows, log_rates = inputs
    length_here = log_rates.shape[-1]
    causal = jnp.arange(length_here)[:, None] >= jnp.arange(length_here)[None, :]
    running_totals = jnp.cumsum(log_rates, axis=-1)
    relative = running_totals[:, :, None] - running_totals[:, None, :]
    weight = jnp.where(causal[None], jnp.exp(jnp.where(causal[None], relative, 0.0)), 0.0)
    score_matrix = (
        jnp.einsum("hqd,hkd->hqk", queries, key_matrix_rows, precision=exact_result) * weight
    )
    carried_state = jnp.einsum(
        "hqd,hdv->hqv",
        queries * jnp.exp(running_totals)[:, :, None],
        memory_state,
        precision=exact_result,
    )
    output_rows = (
        jnp.einsum("arf,afu->aru", score_matrix, value_matrix_rows, precision=exact_result)
        + carried_state
    )
    decay_factors = jnp.exp(running_totals[:, -1:] - running_totals)
    memory_state = memory_state * jnp.exp(running_totals[:, -1])[:, None, None] + jnp.einsum(
        "iwj,iwe->ije",
        key_matrix_rows * decay_factors[:, :, None],
        value_matrix_rows,
        precision=exact_result,
    )
    return (memory_state, output_rows)


def chain(earlier, later):
    return (earlier[0] * later[0], earlier[1] * later[0][:, None, None] + later[1])


def shards(
    tokens,
    norm_gain,
    ret_query,
    ret_key,
    ret_value,
    att_query,
    att_key,
    att_value,
    log_decay,
    start_state,
    ret_gain,
    sink_logits,
    ret_out,
    att_out,
):
    gathered = lax.all_gather(tokens[0], "tp", axis=1, tiled=True)
    row_count = gathered.shape[0]
    as_float = gathered.astype(jnp.float32)
    normed = (
        as_float
        * lax.rsqrt(jnp.mean(as_float * as_float, axis=-1, keepdims=True) + epsilon)
        * norm_gain
    ).astype(jnp.bfloat16)
    offset = lax.axis_index("sp") * row_count
    positions = offset + jnp.arange(row_count, dtype=jnp.int32)
    weights = (ret_query, ret_key, ret_value, att_query, att_key, att_value)
    pieces = (
        lax.all_gather(weights[0], "sp", axis=0, tiled=True),
        lax.all_gather(weights[1], "sp", axis=0, tiled=True),
        lax.all_gather(weights[2], "sp", axis=0, tiled=True),
        lax.all_gather(weights[3], "sp", axis=0, tiled=True),
        lax.all_gather(weights[4], "sp", axis=0, tiled=True),
        lax.all_gather(weights[5], "sp", axis=0, tiled=True),
    )
    projected = tuple(
        (jnp.dot(normed, piece, preferred_element_type=jnp.float32) for piece in pieces)
    )
    rounded = tuple((product_f.astype(jnp.bfloat16) for product_f in projected))
    projected = rounded[:3]
    head_count = projected[0].shape[1] // DK
    queries = rotate(projected[0].astype(jnp.float32).reshape(row_count, head_count, DK), positions)
    keys_rot = rotate(
        projected[1].astype(jnp.float32).reshape(row_count, head_count, DK), positions
    ) * DK ** (-0.5)
    values_f = projected[2].astype(jnp.float32).reshape(row_count, head_count, DV)
    log_rates = log_decay[0]
    count = row_count // BLOCK

    def blocked(array):
        return array.reshape(count, BLOCK, head_count, array.shape[-1]).transpose(0, 2, 1, 3)

    rates_blocked = log_rates.reshape(head_count, count, BLOCK).transpose(1, 0, 2)
    local_state, pieces = lax.scan(
        block_step,
        jnp.zeros((head_count, DK, DV), jnp.float32),
        (blocked(queries), blocked(keys_rot), blocked(values_f), rates_blocked),
    )
    local_out = pieces.transpose(0, 2, 1, 3).reshape(row_count, head_count, DV)
    running_totals = jnp.cumsum(log_rates, axis=-1)
    device_decay = jnp.exp(running_totals[:, -1])
    identity = (jnp.ones((head_count,), jnp.float32), jnp.zeros((head_count, DK, DV), jnp.float32))
    prior_decay, prior_state = carried_in((device_decay, local_state), "sp", chain, identity)
    incoming = prior_state + prior_decay[:, None, None] * start_state[0]
    retained = local_out + jnp.einsum(
        "thd,hdv->thv",
        queries * jnp.exp(running_totals).T[:, :, None],
        incoming,
        precision=exact_result,
    )
    centred = retained - jnp.mean(retained, axis=-1, keepdims=True)
    variance = jnp.mean(centred * centred, axis=-1, keepdims=True)
    ret_hidden = (
        (centred * lax.rsqrt(variance + epsilon)).reshape(row_count, head_count * DV) * ret_gain
    ).astype(jnp.bfloat16)
    att_queries, att_keys, att_values = rounded[3:]
    kv_heads = att_keys.shape[1] // HD
    groups = att_queries.shape[1] // HD // kv_heads
    earlier_keys, earlier_values = passed_along(
        (att_keys[row_count - WINDOW :], att_values[row_count - WINDOW :]), "sp", 1
    )
    extended_keys = jnp.concatenate([earlier_keys, att_keys], axis=0)
    extended_values = jnp.concatenate([earlier_values, att_values], axis=0)
    windows = row_count // WINDOW

    def banded(array):
        earlier = array[:row_count].reshape(windows, WINDOW, kv_heads, HD)
        current = array[WINDOW:].reshape(windows, WINDOW, kv_heads, HD)
        return jnp.concatenate([earlier, current], axis=1)

    key_band = banded(extended_keys)
    value_band = banded(extended_values)
    grouped_q = att_queries.reshape(windows, WINDOW, kv_heads, groups, HD)
    score_matrix = jnp.einsum(
        "nqhgd,nkhd->nhgqk", grouped_q, key_band, preferred_element_type=jnp.float32
    ) * HD ** (-0.5)
    query_index = WINDOW + jnp.arange(WINDOW)
    key_index = jnp.arange(2 * WINDOW)
    allowed = (key_index[None, :] <= query_index[:, None]) & (
        query_index[:, None] - key_index[None, :] < WINDOW
    )
    key_place = offset - WINDOW + jnp.arange(windows)[:, None] * WINDOW + key_index[None, :]
    visible = (allowed[None] & (key_place >= 0)[:, None, :])[:, None, None]
    expo = jnp.exp(jnp.where(visible, score_matrix, -1e30))
    summed = jnp.sum(expo, axis=-1, keepdims=True) + jnp.exp(sink_logits).reshape(
        1, kv_heads, groups, 1, 1
    )
    probs = (expo / summed).astype(jnp.bfloat16)
    attended = jnp.einsum(
        "nhgqk,nkhd->nqhgd", probs, value_band, preferred_element_type=jnp.float32
    )
    att_hidden = attended.astype(jnp.bfloat16).reshape(row_count, kv_heads * groups * HD)
    ret_width = ret_hidden.shape[1]
    joined = jnp.concatenate([ret_hidden, att_hidden], axis=1)[None]
    piece = lax.all_gather(joined, "fs", axis=0, tiled=True)
    product = jnp.einsum(
        "srh,hd->srd", piece[:, :, :ret_width], ret_out, preferred_element_type=jnp.float32
    )
    product = product + jnp.einsum(
        "srh,hd->srd", piece[:, :, ret_width:], att_out, preferred_element_type=jnp.float32
    )
    partial_rows = product.astype(jnp.bfloat16)
    regrouped = lax.all_to_all(partial_rows, "fs", split_axis=0, concat_axis=2, tiled=True)
    mixed = lax.psum_scatter(
        regrouped[0].astype(jnp.float32).astype(jnp.bfloat16), "tp", scatter_dimension=1, tiled=True
    )
    return mixed[None]


MESH = pl.DeviceIdType.MESH
F32 = jnp.float32
BF16 = jnp.bfloat16
GAIN_ROW = 0
DECAY_ROW = 1
SINK_ROW = 8


def dot(a, b):
    return jnp.dot(a, b, preferred_element_type=F32)


def dot_t(a, b):
    return lax.dot_general(a, b, (((1,), (1,)), ((), ())), preferred_element_type=F32)


def dot_l(a, b):
    return lax.dot_general(a, b, (((0,), (0,)), ((), ())), preferred_element_type=F32)


def fused(
    n_sp, n_fs, tok_in, ngain_in, rq, rk, rv, aq, ak, av, gain_in, decay_in, sink_in, start, ro, ao, cos_in, sin_in, out,
    tok, ngain, small, cos, sin, gain_v, decay_v, sink_v, insem,
    toks, ss_mine, ss_peer, w, wo, sm, s0, proj, kv, hid, hin, state,
    send, wsem, wpsem, smsem, ssem, sssem, tsem, osem, hsem, lsem,
):
    z, f, c = lax.axis_index("sp"), lax.axis_index("fs"), lax.axis_index("tp")
    peer = 1 - c
    inputs = [
        pltpu.make_async_copy(src, dst, insem.at[i])
        for i, (src, dst) in enumerate(
            ((tok_in, tok), (ngain_in, ngain), (gain_in, gain_v), (decay_in, decay_v),
             (sink_in, sink_v), (cos_in, cos), (sin_in, sin))
        )
    ]
    for copy in inputs:
        copy.start()
    rows, half = tok.shape
    depth = rq.shape[0]
    quarter = depth // n_fs
    heads_core = rq.shape[1] // DK
    kvw = ak.shape[1]
    groups = aq.shape[1] // kvw
    qw = groups * HD
    ret_cols, att_cols = 3 * DK, qw + 2 * kvw
    sub = lax.rem(z, heads_core)
    is0, is1 = c == 0, c == 1

    barrier = pltpu.get_barrier_semaphore()
    count = 0

    def greet(**where):
        pl.semaphore_signal(barrier, inc=1, device_id=where, device_id_type=MESH)

    greet(tp=peer)
    for t in range(2):
        for i in range(1, n_sp):
            greet(sp=lax.rem(z + i, n_sp), tp=jnp.int32(t))
            count += 1
        for i in range(1, n_fs):
            greet(fs=lax.rem(f + i, n_fs), tp=jnp.int32(t))
            count += 1
    pl.semaphore_wait(barrier, count + 1)

    sent = []
    slots = iter(range(send.shape[0]))

    def both(a, b):
        if a is None:
            return b
        return a if b is None else jnp.logical_and(a, b)

    def remote(cond, src, dst, rsem, slot=None, **where):
        slot = next(slots) if slot is None else slot
        copy = pltpu.make_async_remote_copy(
            src_ref=src, dst_ref=dst, send_sem=send.at[slot], recv_sem=rsem,
            device_id=where, device_id_type=MESH,
        )
        sent.append((cond, copy))
        if cond is None:
            copy.start()
        else:
            pl.when(cond)(copy.start)

    def local(cond, src, dst, sem):
        pl.when(cond)(pltpu.make_async_copy(src, dst, sem).start)

    def arrived(dst, sem):
        pltpu.make_async_copy(dst, dst, sem).wait()

    def wrows(at, n):
        return pl.ds(pl.multiple_of(at, quarter), n)

    for copy in inputs[2:5]:
        copy.wait()
    small[...] = jnp.zeros_like(small)
    small[pl.ds(GAIN_ROW, 1), pl.ds(0, gain_v.shape[1])] = gain_v[...]
    for j in range(heads_core):
        small[pl.ds(DECAY_ROW, 1), pl.ds(j * rows, rows)] = decay_v[pl.ds(j, 1), :]
    n_sink = sink_v.shape[1]
    diagonal = lax.broadcasted_iota(jnp.int32, (n_sink, n_sink), 0) == lax.broadcasted_iota(
        jnp.int32, (n_sink, n_sink), 1
    )
    column = jnp.sum(jnp.where(diagonal, sink_v[...], 0.0), axis=1, keepdims=True)
    small[pl.ds(SINK_ROW, n_sink), :] = jnp.broadcast_to(column, (n_sink, small.shape[1]))

    def pieces(j, kind):
        if kind == 0:
            return [(a, pl.ds(j * DK, DK), pl.ds(i * DK, DK)) for i, a in enumerate((rq, rk, rv))]
        return [
            (aq, pl.ds(j * qw, qw), pl.ds(0, qw)),
            (ak, pl.ds(0, kvw), pl.ds(qw, kvw)),
            (av, pl.ds(0, kvw), pl.ds(qw + kvw, kvw)),
        ]

    mine = pl.ds(pl.multiple_of(f * quarter, quarter), quarter)
    for j in range(heads_core):
        p = heads_core * c + j
        away = p != z
        here = p == z
        for kind in range(2):
            remote(away, small, sm.at[z], smsem.at[z], sp=p, tp=jnp.int32(kind))
            for i, (a, cs, cd) in enumerate(pieces(j, kind)):
                remote(
                    away, a.at[mine, cs], w.at[wrows(z * depth + f * quarter, quarter), cd],
                    wsem.at[z, i], sp=p, tp=jnp.int32(kind),
                )
        remote(here, small, sm.at[z], smsem.at[z], tp=peer)
        local(here, small, sm.at[z], smsem.at[z])
        for kind in range(2):
            same, other = both(here, c == kind), both(here, c != kind)
            for i, (a, cs, cd) in enumerate(pieces(j, kind)):
                dst = w.at[wrows(z * depth, depth), cd]
                local(same, a.at[:, cs], dst, wsem.at[z, i])
                remote(other, a.at[:, cs], dst, wsem.at[z, i], tp=peer)
        local(both(here, is0), start.at[j], s0, ssem)
        remote(both(here, is1), start.at[j], s0, ssem, tp=peer)

    fs_core = n_fs // 2
    owner = f // fs_core
    out_rows, out_cols = ro.shape

    def out_block(kind, core, fsrc):
        j = lax.rem(fsrc, fs_core)
        block = wo.at[kind, pl.ds(pl.multiple_of(core * out_rows, out_rows), out_rows),
                      pl.ds(pl.multiple_of(j * out_cols, out_cols), out_cols)]
        return block, osem.at[kind, core, j]

    beside, across = f + 1 - 2 * lax.rem(f, 2), lax.rem(f + 2, n_fs)
    corner = lax.rem(beside + 2, n_fs)

    def send_out(kind):
        a = (ro, ao)[kind]
        dst, sem = out_block(kind, c, f)
        remote(None, a, dst, sem, fs=beside, tp=owner)
        remote(None, a, dst, sem, fs=across, tp=owner)
        local(c == owner, a, dst, sem)
        remote(c != owner, a, dst, sem, tp=peer)

    def pass_out(kind):
        cond, fsrc, to = ((c == owner, beside, across), (c != owner, across, beside))[kind]
        for core in range(2):
            block, sem = out_block(kind, core, fsrc)
            pl.when(cond)(functools.partial(arrived, block, sem))
            remote(cond, block, block, sem, fs=to)

    send_out(0)

    inputs[0].wait()
    inputs[1].wait()
    x = tok[...].astype(F32)
    sq = x * x
    part = sq[:, :128]
    for i in range(1, half // 128):
        part = part + sq[:, i * 128 : (i + 1) * 128]
    ss_mine[...] = part
    remote(None, ss_mine, ss_peer, sssem, tp=peer)
    arrived(ss_peer, sssem)
    mean = jnp.sum(ss_mine[...] + ss_peer[...], axis=-1, keepdims=True) / (2 * half)
    scale = lax.rsqrt(mean + epsilon)
    g = ngain[:, pl.ds(pl.multiple_of(c * half, 128), half)]
    toks[z, c] = (tok[...].astype(F32) * scale * g).astype(BF16)

    def spread(zs, cond, up, down):
        block = toks.at[zs, c]
        if up is not None:
            remote(both(cond, up), block, block, tsem.at[zs, c], sp=lax.rem(z + 1, n_sp))
        if down is not None:
            remote(both(cond, down), block, block, tsem.at[zs, c], sp=lax.rem(z + n_sp - 1, n_sp))
        remote(cond, block, block, tsem.at[zs, c], tp=peer)

    spread(z, None, z < n_sp - 1, z > 0)

    def widths(act):
        for kind, cols in ((0, ret_cols), (1, att_cols)):
            act(c == kind, pl.ds(0, cols))

    for i in range(1, n_sp):
        zs = lax.rem(z + i, n_sp)
        at = wrows(zs * depth + f * quarter, quarter)
        for kind in range(2):
            @pl.when(c == kind)
            def _():
                for n, (_, _, cd) in enumerate(pieces(0, kind)):
                    arrived(w.at[at, cd], wsem.at[zs, n])
        base = [next(slots) for _ in range(n_fs - 1)]
        for kind, cols in ((0, ret_cols), (1, att_cols)):
            for k in range(1, n_fs):
                block = w.at[at, pl.ds(0, cols)]
                remote(c == kind, block, block, wpsem.at[zs, f], slot=base[k - 1],
                       fs=lax.rem(f + k, n_fs))

    send_out(1)

    for i in range(n_sp):
        arrived(sm.at[i], smsem.at[i])
    kv[pl.ds(0, WINDOW), :] = jnp.zeros((WINDOW, kv.shape[1]), BF16)

    def project(zs):
        at = pl.ds(pl.multiple_of(zs * rows, rows), rows)

        def tile(cols):
            return dot(toks[zs, 0], w[pl.ds(0, half), cols]) + dot(toks[zs, 1], w[pl.ds(half, half), cols])

        @pl.when(is0)
        def _():
            @pl.loop(0, 3)
            def _(i):
                cols = pl.ds(pl.multiple_of(i * DK, DK), DK)
                proj[at, cols] = tile(cols).astype(BF16)

            co, si = cos[at, :], sin[at, :]
            h = DK // 2
            for i, factor in ((0, 1.0), (1, DK ** (-0.5))):
                a = proj[at, pl.ds(i * DK, h)].astype(F32)
                b = proj[at, pl.ds(i * DK + h, h)].astype(F32)
                proj[at, pl.ds(i * DK, h)] = ((a * co - b * si) * factor).astype(BF16)
                proj[at, pl.ds(i * DK + h, h)] = ((a * si + b * co) * factor).astype(BF16)

        @pl.when(is1)
        def _():
            proj[at, pl.ds(0, qw)] = tile(pl.ds(0, qw)).astype(BF16)
            both_kv = tile(pl.ds(qw, 2 * kvw))
            to = pl.ds(pl.multiple_of(WINDOW + zs * rows, WINDOW), rows)
            for n in range(2):
                got = both_kv[:, n * kvw : n * kvw + HD]
                for s in range(1, heads_core):
                    got = jnp.where(sub == s, both_kv[:, n * kvw + s * HD : n * kvw + (s + 1) * HD], got)
                kv[to, pl.ds(n * 128, HD)] = got.astype(BF16)

    lane = lax.broadcasted_iota(jnp.int32, (BLOCK, BLOCK), 1)
    row = lax.broadcasted_iota(jnp.int32, (BLOCK, BLOCK), 0)
    per = rows // BLOCK

    def retention(p, i):
        b = p * per + i
        at = pl.ds(pl.multiple_of(b * BLOCK, BLOCK), BLOCK)
        l = sm[p, pl.ds(DECAY_ROW, 1), pl.ds(pl.multiple_of(sub * rows + i * BLOCK, BLOCK), BLOCK)]
        cum = jnp.sum(jnp.where(lane <= row, l, 0.0), axis=1, keepdims=True)
        cum_row = jnp.sum(jnp.where(lane == row, cum, 0.0), axis=0, keepdims=True)
        total = jnp.sum(l, axis=1, keepdims=True)
        weight = jnp.where(lane <= row, jnp.exp(jnp.where(lane <= row, cum - cum_row, 0.0)), 0.0)
        q, k, v = (proj[at, pl.ds(n * DK, DK)] for n in range(3))
        st = state[...]
        scores = (dot_t(q, k) * weight).astype(BF16)
        o = dot(scores, v) + dot((q.astype(F32) * jnp.exp(cum)).astype(BF16), st.astype(BF16))
        kd = (k.astype(F32) * jnp.exp(total - cum)).astype(BF16)
        state[...] = st * jnp.exp(total) + dot_l(kd, v)
        centred = o - jnp.mean(o, axis=-1, keepdims=True)
        var = jnp.mean(centred * centred, axis=-1, keepdims=True)
        gain = sm[z, pl.ds(GAIN_ROW, 1), pl.ds(pl.multiple_of(sub * DV, DV), DV)]
        hid[at, :] = (centred * lax.rsqrt(var + epsilon) * gain).astype(BF16)

    lane2 = lax.broadcasted_iota(jnp.int32, (WINDOW, 2 * WINDOW), 1)
    row2 = lax.broadcasted_iota(jnp.int32, (WINDOW, 2 * WINDOW), 0)

    def attention(b):
        at = pl.ds(pl.multiple_of(b * WINDOW, WINDOW), WINDOW)
        band = pl.ds(pl.multiple_of(b * WINDOW, WINDOW), 2 * WINDOW)
        k, v = kv[band, pl.ds(0, HD)], kv[band, pl.ds(128, HD)]
        visible = (lane2 <= row2 + WINDOW) & (lane2 > row2) & (lane2 + b * WINDOW >= WINDOW)
        sinks = sm[z, pl.ds(SINK_ROW, heads_core * groups), pl.ds(0, 128)]
        res = []
        for h in range(groups):
            q = proj[at, pl.ds(h * HD, HD)]
            score = dot_t(q, k) * HD ** (-0.5)
            e = jnp.exp(jnp.where(visible, score, -1e30))
            logit = sinks[h : h + 1, :1]
            for s in range(1, heads_core):
                logit = jnp.where(sub == s, sinks[s * groups + h : s * groups + h + 1, :1], logit)
            sink = jnp.exp(logit)
            total = jnp.sum(e, axis=-1, keepdims=True) + sink
            res.append(dot((e / total).astype(BF16), v))
        hid[at, :] = jnp.concatenate(res, axis=1).astype(BF16)

    def all_weights():
        for kind, cols in ((0, ret_cols), (1, att_cols)):
            @pl.when(c == kind)
            def _():
                for n, (_, _, cd) in enumerate(pieces(0, kind)):
                    arrived(w.at[wrows(z * depth, depth), cd], wsem.at[z, n])
                for i in range(1, n_sp):
                    zs = lax.rem(z + i, n_sp)
                    for k in range(1, n_fs):
                        fs = lax.rem(f + k, n_fs)
                        arrived(w.at[wrows(zs * depth + fs * quarter, quarter), pl.ds(0, cols)],
                                wpsem.at[zs, fs])

    def hand_on(p, cond):
        block = hid.at[pl.ds(pl.multiple_of(p * rows, rows), rows)]
        remote(both(cond, p != z), block, hin.at[c, z], hsem.at[c, z], sp=p)
        local(both(cond, p == z), block, hin.at[c, z], hsem.at[c, z])

    def land(d):
        for s in (-1, 1):
            zs = z + s * d
            ok = zs >= 0 if s < 0 else zs < n_sp
            zs = jnp.clip(zs, 0, n_sp - 1)
            pl.when(ok)(functools.partial(arrived, toks.at[zs, c], tsem.at[zs, c]))
            if s < 0:
                spread(zs, ok, z < n_sp - 1, None)
            else:
                spread(zs, ok, None, z > 0)

    def attend(first, last):
        @pl.loop(first * per, last * per)
        def _(b):
            attention(b)

    def take(d):
        for s in (-1, 1) if d else (0,):
            zs = z + s * d
            ok = jnp.logical_and(zs >= 0, zs < n_sp)
            zs = jnp.clip(zs, 0, n_sp - 1)

            @pl.when(ok)
            def _():
                arrived(toks.at[zs, peer], tsem.at[zs, peer])
                project(zs)

            first = both(ok, both(is1, zs == 0))
            if s > 0:
                pl.when(both(ok, is1))(functools.partial(attend, zs, zs + 1))
                hand_on(zs, both(ok, is1))
            elif s < 0:
                pl.when(both(ok, is1))(
                    functools.partial(attend, zs + jnp.where(zs == 0, 0, 1), zs + 2)
                )
                hand_on(zs + 1, both(ok, is1))
                hand_on(jnp.int32(0), first)
            else:
                pl.when(first)(functools.partial(attend, zs, zs + 1))
                hand_on(jnp.int32(0), first)

    for d in range(1, n_sp - 1):
        land(d)
    inputs[5].wait()
    inputs[6].wait()
    all_weights()
    pass_out(0)
    for d in range(n_sp - 1):
        take(d)
    land(n_sp - 1)
    take(n_sp - 1)
    pass_out(1)

    @pl.when(is0)
    def _():
        arrived(s0, ssem)
        state[...] = s0[...]

    for p in range(n_sp):
        @pl.when(is0)
        def _():
            pl.loop(0, per)(functools.partial(retention, p))

        hand_on(jnp.int32(p), is0)

    for i in range(n_sp):
        zs = lax.rem(z + i, n_sp)
        arrived(hin.at[c, zs], hsem.at[c, zs])
        remote(None, hin.at[c, zs], hin.at[c, zs], hsem.at[c, zs], tp=peer)
    for kind in range(2):
        for cs in range(2):
            for j in range(fs_core):
                block, sem = out_block(kind, cs, jnp.int32(j))
                passed = both(c == owner, beside == c * fs_core + j) if kind == 0 else both(
                    c != owner, across == c * fs_core + j
                )
                pl.when(jnp.logical_not(passed))(functools.partial(arrived, block, sem))
    for zs in range(n_sp):
        arrived(hin.at[peer, zs], hsem.at[peer, zs])

    @pl.loop(0, out.shape[1] // 256)
    def _(i):
        cols = pl.ds(pl.multiple_of(i * 256, 256), 256)
        acc = None
        for kind in range(2):
            for h in range(n_sp):
                width = hin.shape[3]
                term = dot(hin[kind, h], wo[kind, pl.ds(h * width, width), cols])
                acc = term if acc is None else acc + term
        out[:, cols] = acc.astype(BF16)

    for cond, copy in sent:
        if cond is None:
            copy.wait_send()
        else:
            pl.when(cond)(copy.wait_send)


def layer(mesh, *args):
    (tokens, norm_gain, ret_query, ret_key, ret_value, att_query, att_key, att_value,
     log_decay, start_state, ret_gain, sink_logits, ret_out, att_out) = args
    n_sp, n_fs, n_tp = mesh.shape["sp"], mesh.shape["fs"], mesh.shape["tp"]
    heads = ret_query.shape[1] // DK
    kv_heads = att_key.shape[1] // HD
    rows, half = tokens.shape[1:]
    whole_heads = (
        n_tp == 2 and n_fs == 4 and heads * n_tp == n_sp and kv_heads == heads
        and att_query.shape[1] == ret_query.shape[1]
    )
    if not whole_heads:
        return shards(*args)
    depth = ret_query.shape[0]
    wide = heads * rows
    small = (SINK_ROW + sink_logits.shape[0], wide)
    h = DK // 2
    inverse = np.float32(1.0) / np.float32(10000.0) ** (np.arange(h, dtype=np.float32) / np.float32(h))
    angles = np.arange(n_sp * rows, dtype=np.float32)[:, None] * inverse[None, :]
    cos = jnp.asarray(np.cos(angles), F32)
    sin = jnp.asarray(np.sin(angles), F32)
    length = n_sp * rows
    vm = pl.BlockSpec(memory_space=pltpu.VMEM)
    hbm = pl.BlockSpec(memory_space=pl.ANY)
    dma = pltpu.SemaphoreType.DMA
    res = pl.pallas_call(
        functools.partial(fused, n_sp, n_fs),
        out_shape=jax.ShapeDtypeStruct((rows, half), BF16),
        in_specs=[hbm] * 16,
        out_specs=vm,
        scratch_shapes=[
            pltpu.VMEM((rows, half), BF16),
            pltpu.VMEM((1, norm_gain.shape[0]), F32),
            pltpu.VMEM(small, F32),
            pltpu.VMEM((length, h), F32),
            pltpu.VMEM((length, h), F32),
            pltpu.VMEM((1, ret_gain.shape[0]), F32),
            pltpu.VMEM((heads, rows), F32),
            pltpu.VMEM((1, sink_logits.shape[0]), F32),
            dma((7,)),
            pltpu.VMEM((n_sp, 2, rows, half), BF16),
            pltpu.VMEM((rows, 128), F32),
            pltpu.VMEM((rows, 128), F32),
            pltpu.VMEM((n_sp * depth, 3 * DK), BF16),
            pltpu.VMEM((2, 2 * ret_out.shape[0], n_fs // 2 * ret_out.shape[1]), BF16),
            pltpu.VMEM((n_sp,) + small, F32),
            pltpu.VMEM((DK, DV), F32),
            pltpu.VMEM((length, 3 * DK), BF16),
            pltpu.VMEM((WINDOW + length, 256), BF16),
            pltpu.VMEM((length, DV), BF16),
            pltpu.VMEM((2, n_sp, rows, DV), BF16),
            pltpu.VMEM((DK, DV), F32),
            dma((100,)),
            dma((n_sp, 3)),
            dma((n_sp, n_fs)),
            dma((n_sp,)),
            dma,
            dma,
            dma((n_sp, 2)),
            dma((2, 2, n_fs // 2)),
            dma((2, n_sp)),
            dma,
        ],
        compiler_params=pltpu.CompilerParams(
            collective_id=0, has_side_effects=True, vmem_limit_bytes=67043328
        ),
    )(
        tokens[0], norm_gain[None], ret_query, ret_key, ret_value, att_query, att_key, att_value,
        ret_gain[None], log_decay[0], sink_logits[None], start_state[0], ret_out, att_out, cos, sin,
    )
    return res[None]


def solution(mesh):
    placed = (
        P("fs", "sp", "tp"),
        P(),
        P("sp", "tp"),
        P("sp", "tp"),
        P("sp", "tp"),
        P("sp", "tp"),
        P("sp", "tp"),
        P("sp", "tp"),
        P("fs", "tp", "sp"),
        P("fs", "tp", None, None),
        P("tp"),
        P("tp"),
        P("tp", "fs"),
        P("tp", "fs"),
    )
    return jax.shard_map(
        functools.partial(layer, mesh), mesh=mesh, in_specs=placed, out_specs=P("fs", "sp", "tp"), check_vma=False
    )
```

```python
import functools

import jax
import jax.numpy as jnp
import numpy as np
from jax import lax
from jax.experimental import pallas as pl
from jax.experimental.pallas import tpu as pltpu
from jax.sharding import PartitionSpec as P

DK = 256
DV = 256
HD = 64
WINDOW = 128
BLOCK = 128


epsilon = 1e-06
exact_result = lax.Precision.HIGHEST


def carried_in(array, axis, combine, identity):
    peers, mine = (lax.axis_size(axis), lax.axis_index(axis))
    everything = jax.tree.map(
        lambda part, kind: lax.all_gather(part.astype(kind), axis),
        array,
        (jnp.bfloat16, jnp.bfloat16),
    )
    start = jax.tree.map(
        lambda part, zero: jnp.broadcast_to(jnp.asarray(zero, part.dtype), part.shape),
        array,
        identity,
    )

    def hop(k, before):
        reached = k < mine
        new = combine(
            before, jax.tree.map(lambda part, own: part[k].astype(own.dtype), everything, array)
        )
        return jax.tree.map(lambda a, b: jnp.where(reached, a, b), new, before)

    return lax.fori_loop(0, peers, hop, start)


def passed_along(block, axis, distance):
    devices = range(lax.axis_size(axis))
    route = [(i - distance, i) for i in devices if i - distance in devices]
    return lax.ppermute(block, axis, route)


def rotate(values, positions):
    half_dim = values.shape[-1] // 2
    inverse = 1.0 / 10000.0 ** (jnp.arange(half_dim, dtype=jnp.float32) / half_dim)
    angles = positions.astype(jnp.float32)[:, None] * inverse[None, :]
    cosine = jnp.cos(angles)[:, None, :]
    sine_table = jnp.sin(angles)[:, None, :]
    front_half = values[..., :half_dim]
    back_half = values[..., half_dim:]
    return jnp.concatenate(
        [
            front_half * cosine - back_half * sine_table,
            front_half * sine_table + back_half * cosine,
        ],
        axis=-1,
    )


def block_step(memory_state, inputs):
    queries, key_matrix_rows, value_matrix_rows, log_rates = inputs
    length_here = log_rates.shape[-1]
    causal = jnp.arange(length_here)[:, None] >= jnp.arange(length_here)[None, :]
    running_totals = jnp.cumsum(log_rates, axis=-1)
    relative = running_totals[:, :, None] - running_totals[:, None, :]
    weight = jnp.where(causal[None], jnp.exp(jnp.where(causal[None], relative, 0.0)), 0.0)
    score_matrix = (
        jnp.einsum("hqd,hkd->hqk", queries, key_matrix_rows, precision=exact_result) * weight
    )
    carried_state = jnp.einsum(
        "hqd,hdv->hqv",
        queries * jnp.exp(running_totals)[:, :, None],
        memory_state,
        precision=exact_result,
    )
    output_rows = (
        jnp.einsum("arf,afu->aru", score_matrix, value_matrix_rows, precision=exact_result)
        + carried_state
    )
    decay_factors = jnp.exp(running_totals[:, -1:] - running_totals)
    memory_state = memory_state * jnp.exp(running_totals[:, -1])[:, None, None] + jnp.einsum(
        "iwj,iwe->ije",
        key_matrix_rows * decay_factors[:, :, None],
        value_matrix_rows,
        precision=exact_result,
    )
    return (memory_state, output_rows)


def chain(earlier, later):
    return (earlier[0] * later[0], earlier[1] * later[0][:, None, None] + later[1])


def shards(
    tokens,
    norm_gain,
    ret_query,
    ret_key,
    ret_value,
    att_query,
    att_key,
    att_value,
    log_decay,
    start_state,
    ret_gain,
    sink_logits,
    ret_out,
    att_out,
):
    gathered = lax.all_gather(tokens[0], "tp", axis=1, tiled=True)
    row_count = gathered.shape[0]
    as_float = gathered.astype(jnp.float32)
    normed = (
        as_float
        * lax.rsqrt(jnp.mean(as_float * as_float, axis=-1, keepdims=True) + epsilon)
        * norm_gain
    ).astype(jnp.bfloat16)
    offset = lax.axis_index("sp") * row_count
    positions = offset + jnp.arange(row_count, dtype=jnp.int32)
    weights = (ret_query, ret_key, ret_value, att_query, att_key, att_value)
    pieces = (
        lax.all_gather(weights[0], "sp", axis=0, tiled=True),
        lax.all_gather(weights[1], "sp", axis=0, tiled=True),
        lax.all_gather(weights[2], "sp", axis=0, tiled=True),
        lax.all_gather(weights[3], "sp", axis=0, tiled=True),
        lax.all_gather(weights[4], "sp", axis=0, tiled=True),
        lax.all_gather(weights[5], "sp", axis=0, tiled=True),
    )
    projected = tuple(
        (jnp.dot(normed, piece, preferred_element_type=jnp.float32) for piece in pieces)
    )
    rounded = tuple((product_f.astype(jnp.bfloat16) for product_f in projected))
    projected = rounded[:3]
    head_count = projected[0].shape[1] // DK
    queries = rotate(projected[0].astype(jnp.float32).reshape(row_count, head_count, DK), positions)
    keys_rot = rotate(
        projected[1].astype(jnp.float32).reshape(row_count, head_count, DK), positions
    ) * DK ** (-0.5)
    values_f = projected[2].astype(jnp.float32).reshape(row_count, head_count, DV)
    log_rates = log_decay[0]
    count = row_count // BLOCK

    def blocked(array):
        return array.reshape(count, BLOCK, head_count, array.shape[-1]).transpose(0, 2, 1, 3)

    rates_blocked = log_rates.reshape(head_count, count, BLOCK).transpose(1, 0, 2)
    local_state, pieces = lax.scan(
        block_step,
        jnp.zeros((head_count, DK, DV), jnp.float32),
        (blocked(queries), blocked(keys_rot), blocked(values_f), rates_blocked),
    )
    local_out = pieces.transpose(0, 2, 1, 3).reshape(row_count, head_count, DV)
    running_totals = jnp.cumsum(log_rates, axis=-1)
    device_decay = jnp.exp(running_totals[:, -1])
    identity = (jnp.ones((head_count,), jnp.float32), jnp.zeros((head_count, DK, DV), jnp.float32))
    prior_decay, prior_state = carried_in((device_decay, local_state), "sp", chain, identity)
    incoming = prior_state + prior_decay[:, None, None] * start_state[0]
    retained = local_out + jnp.einsum(
        "thd,hdv->thv",
        queries * jnp.exp(running_totals).T[:, :, None],
        incoming,
        precision=exact_result,
    )
    centred = retained - jnp.mean(retained, axis=-1, keepdims=True)
    variance = jnp.mean(centred * centred, axis=-1, keepdims=True)
    ret_hidden = (
        (centred * lax.rsqrt(variance + epsilon)).reshape(row_count, head_count * DV) * ret_gain
    ).astype(jnp.bfloat16)
    att_queries, att_keys, att_values = rounded[3:]
    kv_heads = att_keys.shape[1] // HD
    groups = att_queries.shape[1] // HD // kv_heads
    earlier_keys, earlier_values = passed_along(
        (att_keys[row_count - WINDOW :], att_values[row_count - WINDOW :]), "sp", 1
    )
    extended_keys = jnp.concatenate([earlier_keys, att_keys], axis=0)
    extended_values = jnp.concatenate([earlier_values, att_values], axis=0)
    windows = row_count // WINDOW

    def banded(array):
        earlier = array[:row_count].reshape(windows, WINDOW, kv_heads, HD)
        current = array[WINDOW:].reshape(windows, WINDOW, kv_heads, HD)
        return jnp.concatenate([earlier, current], axis=1)

    key_band = banded(extended_keys)
    value_band = banded(extended_values)
    grouped_q = att_queries.reshape(windows, WINDOW, kv_heads, groups, HD)
    score_matrix = jnp.einsum(
        "nqhgd,nkhd->nhgqk", grouped_q, key_band, preferred_element_type=jnp.float32
    ) * HD ** (-0.5)
    query_index = WINDOW + jnp.arange(WINDOW)
    key_index = jnp.arange(2 * WINDOW)
    allowed = (key_index[None, :] <= query_index[:, None]) & (
        query_index[:, None] - key_index[None, :] < WINDOW
    )
    key_place = offset - WINDOW + jnp.arange(windows)[:, None] * WINDOW + key_index[None, :]
    visible = (allowed[None] & (key_place >= 0)[:, None, :])[:, None, None]
    expo = jnp.exp(jnp.where(visible, score_matrix, -1e30))
    summed = jnp.sum(expo, axis=-1, keepdims=True) + jnp.exp(sink_logits).reshape(
        1, kv_heads, groups, 1, 1
    )
    probs = (expo / summed).astype(jnp.bfloat16)
    attended = jnp.einsum(
        "nhgqk,nkhd->nqhgd", probs, value_band, preferred_element_type=jnp.float32
    )
    att_hidden = attended.astype(jnp.bfloat16).reshape(row_count, kv_heads * groups * HD)
    ret_width = ret_hidden.shape[1]
    joined = jnp.concatenate([ret_hidden, att_hidden], axis=1)[None]
    piece = lax.all_gather(joined, "fs", axis=0, tiled=True)
    product = jnp.einsum(
        "srh,hd->srd", piece[:, :, :ret_width], ret_out, preferred_element_type=jnp.float32
    )
    product = product + jnp.einsum(
        "srh,hd->srd", piece[:, :, ret_width:], att_out, preferred_element_type=jnp.float32
    )
    partial_rows = product.astype(jnp.bfloat16)
    regrouped = lax.all_to_all(partial_rows, "fs", split_axis=0, concat_axis=2, tiled=True)
    mixed = lax.psum_scatter(
        regrouped[0].astype(jnp.float32).astype(jnp.bfloat16), "tp", scatter_dimension=1, tiled=True
    )
    return mixed[None]


MESH = pl.DeviceIdType.MESH
F32 = jnp.float32
BF16 = jnp.bfloat16
GAIN_ROW = 0
DECAY_ROW = 1
SINK_ROW = 8


def dot(a, b):
    return jnp.dot(a, b, preferred_element_type=F32)


def dot_t(a, b):
    return lax.dot_general(a, b, (((1,), (1,)), ((), ())), preferred_element_type=F32)


def dot_l(a, b):
    return lax.dot_general(a, b, (((0,), (0,)), ((), ())), preferred_element_type=F32)


def fused(
    n_sp, n_fs, tok_in, ngain_in, rq, rk, rv, aq, ak, av, gain_in, decay_in, sink_in, start, ro, ao, cos_in, sin_in, out,
    tok, ngain, small, cos, sin, gain_v, decay_v, sink_v, insem,
    toks, ss_mine, ss_peer, w, wo, sm, s0, proj, kv, hid, hin, state, total,
    send, wsem, wpsem, smsem, ssem, sssem, tsem, osem, hsem, lsem,
):
    z, f, c = lax.axis_index("sp"), lax.axis_index("fs"), lax.axis_index("tp")
    peer = 1 - c
    inputs = [
        pltpu.make_async_copy(src, dst, insem.at[i])
        for i, (src, dst) in enumerate(
            ((tok_in, tok), (ngain_in, ngain), (gain_in, gain_v), (decay_in, decay_v),
             (sink_in, sink_v), (cos_in, cos), (sin_in, sin))
        )
    ]
    for copy in inputs:
        copy.start()
    rows, half = tok.shape
    depth = rq.shape[0]
    quarter = depth // n_fs
    heads_core = rq.shape[1] // DK
    kvw = ak.shape[1]
    groups = aq.shape[1] // kvw
    qw = groups * HD
    ret_cols, att_cols = 3 * DK, qw + 2 * kvw
    sub = lax.rem(z, heads_core)
    is0, is1 = c == 0, c == 1

    barrier = pltpu.get_barrier_semaphore()
    count = 0

    def greet(**where):
        pl.semaphore_signal(barrier, inc=1, device_id=where, device_id_type=MESH)

    greet(tp=peer)
    for t in range(2):
        for i in range(1, n_sp):
            greet(sp=lax.rem(z + i, n_sp), tp=jnp.int32(t))
            count += 1
        for i in range(1, n_fs):
            greet(fs=lax.rem(f + i, n_fs), tp=jnp.int32(t))
            count += 1
    pl.semaphore_wait(barrier, count + 1)

    sent = []
    slots = iter(range(send.shape[0]))

    def both(a, b):
        if a is None:
            return b
        return a if b is None else jnp.logical_and(a, b)

    def remote(cond, src, dst, rsem, slot=None, **where):
        slot = next(slots) if slot is None else slot
        copy = pltpu.make_async_remote_copy(
            src_ref=src, dst_ref=dst, send_sem=send.at[slot], recv_sem=rsem,
            device_id=where, device_id_type=MESH,
        )
        sent.append((cond, copy))
        if cond is None:
            copy.start()
        else:
            pl.when(cond)(copy.start)

    def local(cond, src, dst, sem):
        pl.when(cond)(pltpu.make_async_copy(src, dst, sem).start)

    def arrived(dst, sem):
        pltpu.make_async_copy(dst, dst, sem).wait()

    def wrows(at, n):
        return pl.ds(pl.multiple_of(at, quarter), n)

    for copy in inputs[2:5]:
        copy.wait()
    small[...] = jnp.zeros_like(small)
    small[pl.ds(GAIN_ROW, 1), pl.ds(0, gain_v.shape[1])] = gain_v[...]
    for j in range(heads_core):
        small[pl.ds(DECAY_ROW, 1), pl.ds(j * rows, rows)] = decay_v[pl.ds(j, 1), :]
    n_sink = sink_v.shape[1]
    diagonal = lax.broadcasted_iota(jnp.int32, (n_sink, n_sink), 0) == lax.broadcasted_iota(
        jnp.int32, (n_sink, n_sink), 1
    )
    column = jnp.sum(jnp.where(diagonal, sink_v[...], 0.0), axis=1, keepdims=True)
    small[pl.ds(SINK_ROW, n_sink), :] = jnp.broadcast_to(column, (n_sink, small.shape[1]))

    def pieces(j, kind):
        if kind == 0:
            return [(a, pl.ds(j * DK, DK), pl.ds(i * DK, DK)) for i, a in enumerate((rq, rk, rv))]
        return [
            (aq, pl.ds(j * qw, qw), pl.ds(0, qw)),
            (ak, pl.ds(0, kvw), pl.ds(qw, kvw)),
            (av, pl.ds(0, kvw), pl.ds(qw + kvw, kvw)),
        ]

    mine = pl.ds(pl.multiple_of(f * quarter, quarter), quarter)
    for j in range(heads_core):
        p = heads_core * c + j
        away = p != z
        here = p == z
        decay = small.at[pl.ds(0, SINK_ROW)], sm.at[z, pl.ds(0, SINK_ROW)]
        remote(away, *decay, smsem.at[z], sp=p, tp=jnp.int32(0))
        for kind in range(2):
            for i, (a, cs, cd) in enumerate(pieces(j, kind)):
                remote(
                    away, a.at[mine, cs], w.at[wrows(z * depth + f * quarter, quarter), cd],
                    wsem.at[z, i], sp=p, tp=jnp.int32(kind),
                )
        remote(here, small, sm.at[z], smsem.at[z], tp=peer)
        local(here, small, sm.at[z], smsem.at[z])
        for kind in range(2):
            same, other = both(here, c == kind), both(here, c != kind)
            for i, (a, cs, cd) in enumerate(pieces(j, kind)):
                dst = w.at[wrows(z * depth, depth), cd]
                local(same, a.at[:, cs], dst, wsem.at[z, i])
                remote(other, a.at[:, cs], dst, wsem.at[z, i], tp=peer)
        local(both(here, is0), start.at[j], s0, ssem)
        remote(both(here, is1), start.at[j], s0, ssem, tp=peer)

    fs_core = n_fs // 2
    owner = f // fs_core
    out_rows, out_cols = ro.shape

    def out_block(kind, core, fsrc):
        j = lax.rem(fsrc, fs_core)
        block = wo.at[kind, pl.ds(pl.multiple_of(core * out_rows, out_rows), out_rows),
                      pl.ds(pl.multiple_of(j * out_cols, out_cols), out_cols)]
        return block, osem.at[kind, core, j]

    beside, across = f + 1 - 2 * lax.rem(f, 2), lax.rem(f + 2, n_fs)
    corner = lax.rem(beside + 2, n_fs)

    def send_out(kind):
        a = (ro, ao)[kind]
        dst, sem = out_block(kind, c, f)
        remote(None, a, dst, sem, fs=beside, tp=owner)
        remote(None, a, dst, sem, fs=across, tp=owner)
        local(c == owner, a, dst, sem)
        remote(c != owner, a, dst, sem, tp=peer)

    def pass_out(kind):
        cond, fsrc, to = ((c == owner, beside, across), (c != owner, across, beside))[kind]
        for core in range(2):
            block, sem = out_block(kind, core, fsrc)
            pl.when(cond)(functools.partial(arrived, block, sem))
            remote(cond, block, block, sem, fs=to)

    send_out(0)
    send_out(1)

    inputs[0].wait()
    inputs[1].wait()
    x = tok[...].astype(F32)
    sq = x * x
    part = sq[:, :128]
    for i in range(1, half // 128):
        part = part + sq[:, i * 128 : (i + 1) * 128]
    ss_mine[...] = part
    remote(None, ss_mine, ss_peer, sssem, tp=peer)
    arrived(ss_peer, sssem)
    mean = jnp.sum(ss_mine[...] + ss_peer[...], axis=-1, keepdims=True) / (2 * half)
    scale = lax.rsqrt(mean + epsilon)
    g = ngain[:, pl.ds(pl.multiple_of(c * half, 128), half)]
    toks[z, c] = (tok[...].astype(F32) * scale * g).astype(BF16)

    def spread(zs, cond, up, down):
        block = toks.at[zs, c]
        if up is not None:
            remote(both(cond, up), block, block, tsem.at[zs, c], sp=lax.rem(z + 1, n_sp))
        if down is not None:
            remote(both(cond, down), block, block, tsem.at[zs, c], sp=lax.rem(z + n_sp - 1, n_sp))
        remote(cond, block, block, tsem.at[zs, c], tp=peer)

    spread(z, None, z < n_sp - 1, z > 0)

    def widths(act):
        for kind, cols in ((0, ret_cols), (1, att_cols)):
            act(c == kind, pl.ds(0, cols))

    for i in range(1, n_sp):
        zs = lax.rem(jnp.where(z < n_sp // 2, z + i, z + n_sp - i), n_sp)
        at = wrows(zs * depth + f * quarter, quarter)
        for kind in range(2):
            @pl.when(c == kind)
            def _():
                for n, (_, _, cd) in enumerate(pieces(0, kind)):
                    arrived(w.at[at, cd], wsem.at[zs, n])
        base = [next(slots) for _ in range(n_fs - 1)]
        for kind, cols in ((0, ret_cols), (1, att_cols)):
            for k in range(1, n_fs):
                block = w.at[at, pl.ds(0, cols)]
                remote(c == kind, block, block, wpsem.at[zs, f], slot=base[k - 1],
                       fs=lax.rem(f + k, n_fs))

    kv[pl.ds(0, WINDOW), :] = jnp.zeros((WINDOW, kv.shape[1]), BF16)

    def project(zs):
        at = pl.ds(pl.multiple_of(zs * rows, rows), rows)

        def tile(cols):
            return dot(toks[zs, 0], w[pl.ds(0, half), cols]) + dot(toks[zs, 1], w[pl.ds(half, half), cols])

        @pl.when(is0)
        def _():
            @pl.loop(0, 3)
            def _(i):
                cols = pl.ds(pl.multiple_of(i * DK, DK), DK)
                proj[at, cols] = tile(cols).astype(BF16)

            co, si = cos[at, :], sin[at, :]
            h = DK // 2
            for i, factor in ((0, 1.0), (1, DK ** (-0.5))):
                a = proj[at, pl.ds(i * DK, h)].astype(F32)
                b = proj[at, pl.ds(i * DK + h, h)].astype(F32)
                proj[at, pl.ds(i * DK, h)] = ((a * co - b * si) * factor).astype(BF16)
                proj[at, pl.ds(i * DK + h, h)] = ((a * si + b * co) * factor).astype(BF16)

        @pl.when(is1)
        def _():
            proj[at, pl.ds(0, qw)] = tile(pl.ds(0, qw)).astype(BF16)
            both_kv = tile(pl.ds(qw, 2 * kvw))
            to = pl.ds(pl.multiple_of(WINDOW + zs * rows, WINDOW), rows)
            for n in range(2):
                got = both_kv[:, n * kvw : n * kvw + HD]
                for s in range(1, heads_core):
                    got = jnp.where(sub == s, both_kv[:, n * kvw + s * HD : n * kvw + (s + 1) * HD], got)
                kv[to, pl.ds(n * 128, HD)] = got.astype(BF16)

    lane = lax.broadcasted_iota(jnp.int32, (BLOCK, BLOCK), 1)
    row = lax.broadcasted_iota(jnp.int32, (BLOCK, BLOCK), 0)
    per = rows // BLOCK

    def retention(p, i):
        b = p * per + i
        at = pl.ds(pl.multiple_of(b * BLOCK, BLOCK), BLOCK)
        l = sm[p, pl.ds(DECAY_ROW, 1), pl.ds(pl.multiple_of(sub * rows + i * BLOCK, BLOCK), BLOCK)]
        cum = jnp.sum(jnp.where(lane <= row, l, 0.0), axis=1, keepdims=True)
        cum_row = jnp.sum(jnp.where(lane == row, cum, 0.0), axis=0, keepdims=True)
        total = jnp.sum(l, axis=1, keepdims=True)
        weight = jnp.where(lane <= row, jnp.exp(jnp.where(lane <= row, cum - cum_row, 0.0)), 0.0)
        q, k, v = (proj[at, pl.ds(n * DK, DK)] for n in range(3))
        st = state[...]
        scores = (dot_t(q, k) * weight).astype(BF16)
        o = dot(scores, v) + dot((q.astype(F32) * jnp.exp(cum)).astype(BF16), st.astype(BF16))
        kd = (k.astype(F32) * jnp.exp(total - cum)).astype(BF16)
        state[...] = st * jnp.exp(total) + dot_l(kd, v)
        centred = o - jnp.mean(o, axis=-1, keepdims=True)
        var = jnp.mean(centred * centred, axis=-1, keepdims=True)
        gain = sm[z, pl.ds(GAIN_ROW, 1), pl.ds(pl.multiple_of(sub * DV, DV), DV)]
        hid[at, :] = (centred * lax.rsqrt(var + epsilon) * gain).astype(BF16)

    lane2 = lax.broadcasted_iota(jnp.int32, (WINDOW, 2 * WINDOW), 1)
    row2 = lax.broadcasted_iota(jnp.int32, (WINDOW, 2 * WINDOW), 0)

    def attention(b):
        at = pl.ds(pl.multiple_of(b * WINDOW, WINDOW), WINDOW)
        band = pl.ds(pl.multiple_of(b * WINDOW, WINDOW), 2 * WINDOW)
        k, v = kv[band, pl.ds(0, HD)], kv[band, pl.ds(128, HD)]
        visible = (lane2 <= row2 + WINDOW) & (lane2 > row2) & (lane2 + b * WINDOW >= WINDOW)
        sinks = sm[z, pl.ds(SINK_ROW, heads_core * groups), pl.ds(0, 128)]
        res = []
        for h in range(groups):
            q = proj[at, pl.ds(h * HD, HD)]
            score = dot_t(q, k) * HD ** (-0.5)
            e = jnp.exp(jnp.where(visible, score, -1e30))
            logit = sinks[h : h + 1, :1]
            for s in range(1, heads_core):
                logit = jnp.where(sub == s, sinks[s * groups + h : s * groups + h + 1, :1], logit)
            sink = jnp.exp(logit)
            total = jnp.sum(e, axis=-1, keepdims=True) + sink
            res.append(dot((e / total).astype(BF16), v))
        hid[at, :] = jnp.concatenate(res, axis=1).astype(BF16)

    def all_weights():
        for kind, cols in ((0, ret_cols), (1, att_cols)):
            @pl.when(c == kind)
            def _():
                for n, (_, _, cd) in enumerate(pieces(0, kind)):
                    arrived(w.at[wrows(z * depth, depth), cd], wsem.at[z, n])
                for i in range(1, n_sp):
                    zs = lax.rem(z + i, n_sp)
                    for k in range(1, n_fs):
                        fs = lax.rem(f + k, n_fs)
                        arrived(w.at[wrows(zs * depth + fs * quarter, quarter), pl.ds(0, cols)],
                                wpsem.at[zs, fs])

    def hand_on(p, cond):
        block = hid.at[pl.ds(pl.multiple_of(p * rows, rows), rows)]
        remote(both(cond, p != z), block, hin.at[c, z], hsem.at[c, z], sp=p)
        local(both(cond, p == z), block, hin.at[c, z], hsem.at[c, z])

    near = jnp.where(z < n_sp // 2, -1, 1)

    def land(d):
        for s in (near, -near):
            zs, to = z + s * d, z - s
            ok = jnp.logical_and(zs >= 0, zs < n_sp)
            onward = jnp.logical_and(ok, jnp.logical_and(to >= 0, to < n_sp))
            zs, to = jnp.clip(zs, 0, n_sp - 1), jnp.clip(to, 0, n_sp - 1)
            block = toks.at[zs, c]
            pl.when(ok)(functools.partial(arrived, block, tsem.at[zs, c]))
            remote(onward, block, block, tsem.at[zs, c], sp=to)
            remote(ok, block, block, tsem.at[zs, c], tp=peer)

    def attend(first, last):
        @pl.loop(first * per, last * per)
        def _(b):
            attention(b)

    def take(d):
        for s in (-1, 1) if d else (0,):
            zs = z + s * d
            ok = jnp.logical_and(zs >= 0, zs < n_sp)
            zs = jnp.clip(zs, 0, n_sp - 1)

            @pl.when(ok)
            def _():
                arrived(toks.at[zs, peer], tsem.at[zs, peer])
                project(zs)

            first = both(ok, both(is1, zs == 0))
            if s > 0:
                pl.when(both(ok, is1))(functools.partial(attend, zs, zs + 1))
                hand_on(zs, both(ok, is1))
            elif s < 0:
                pl.when(both(ok, is1))(
                    functools.partial(attend, zs + jnp.where(zs == 0, 0, 1), zs + 2)
                )
                hand_on(zs + 1, both(ok, is1))
                hand_on(jnp.int32(0), first)
            else:
                pl.when(first)(functools.partial(attend, zs, zs + 1))
                hand_on(jnp.int32(0), first)

    for d in range(1, n_sp - 1):
        land(d)
    arrived(sm.at[z], smsem.at[z])
    for i in range(1, n_sp):
        zs = lax.rem(z + i, n_sp)
        pl.when(is0)(functools.partial(arrived, sm.at[zs, pl.ds(0, SINK_ROW)], smsem.at[zs]))
    inputs[5].wait()
    inputs[6].wait()
    all_weights()
    pass_out(0)
    pass_out(1)
    for d in range(n_sp - 1):
        take(d)
    land(n_sp - 1)
    take(n_sp - 1)

    @pl.when(is0)
    def _():
        arrived(s0, ssem)
        state[...] = s0[...]

    for p in range(n_sp):
        @pl.when(is0)
        def _():
            pl.loop(0, per)(functools.partial(retention, p))

        hand_on(jnp.int32(p), is0)

    width = hin.shape[3]
    for kind in (1, 0):
        for i in range(n_sp):
            zs = lax.rem(z + i, n_sp)
            block = hin.at[kind, zs]
            arrived(block, hsem.at[kind, zs])
            remote(c == kind, block, block, hsem.at[kind, zs], tp=peer)
        for cs in range(2):
            for j in range(fs_core):
                block, sem = out_block(kind, cs, jnp.int32(j))
                passed = both(c == owner, beside == c * fs_core + j) if kind == 0 else both(
                    c != owner, across == c * fs_core + j
                )
                pl.when(jnp.logical_not(passed))(functools.partial(arrived, block, sem))

        @pl.loop(0, out.shape[1] // 256)
        def _(i):
            cols = pl.ds(pl.multiple_of(i * 256, 256), 256)
            acc = total[:, cols] if kind == 0 else None
            for h in range(n_sp):
                term = dot(hin[kind, h], wo[kind, pl.ds(h * width, width), cols])
                acc = term if acc is None else acc + term
            if kind == 0:
                out[:, cols] = acc.astype(BF16)
            else:
                total[:, cols] = acc

    for cond, copy in sent:
        if cond is None:
            copy.wait_send()
        else:
            pl.when(cond)(copy.wait_send)


def layer(mesh, *args):
    (tokens, norm_gain, ret_query, ret_key, ret_value, att_query, att_key, att_value,
     log_decay, start_state, ret_gain, sink_logits, ret_out, att_out) = args
    n_sp, n_fs, n_tp = mesh.shape["sp"], mesh.shape["fs"], mesh.shape["tp"]
    heads = ret_query.shape[1] // DK
    kv_heads = att_key.shape[1] // HD
    rows, half = tokens.shape[1:]
    whole_heads = (
        n_tp == 2 and n_fs == 4 and heads * n_tp == n_sp and kv_heads == heads
        and att_query.shape[1] == ret_query.shape[1]
    )
    if not whole_heads:
        return shards(*args)
    depth = ret_query.shape[0]
    wide = heads * rows
    small = (SINK_ROW + sink_logits.shape[0], wide)
    h = DK // 2
    inverse = np.float32(1.0) / np.float32(10000.0) ** (np.arange(h, dtype=np.float32) / np.float32(h))
    angles = np.arange(n_sp * rows, dtype=np.float32)[:, None] * inverse[None, :]
    cos = jnp.asarray(np.cos(angles), F32)
    sin = jnp.asarray(np.sin(angles), F32)
    length = n_sp * rows
    vm = pl.BlockSpec(memory_space=pltpu.VMEM)
    hbm = pl.BlockSpec(memory_space=pl.ANY)
    dma = pltpu.SemaphoreType.DMA
    res = pl.pallas_call(
        functools.partial(fused, n_sp, n_fs),
        out_shape=jax.ShapeDtypeStruct((rows, half), BF16),
        in_specs=[hbm] * 16,
        out_specs=vm,
        scratch_shapes=[
            pltpu.VMEM((rows, half), BF16),
            pltpu.VMEM((1, norm_gain.shape[0]), F32),
            pltpu.VMEM(small, F32),
            pltpu.VMEM((length, h), F32),
            pltpu.VMEM((length, h), F32),
            pltpu.VMEM((1, ret_gain.shape[0]), F32),
            pltpu.VMEM((heads, rows), F32),
            pltpu.VMEM((1, sink_logits.shape[0]), F32),
            dma((7,)),
            pltpu.VMEM((n_sp, 2, rows, half), BF16),
            pltpu.VMEM((rows, 128), F32),
            pltpu.VMEM((rows, 128), F32),
            pltpu.VMEM((n_sp * depth, 3 * DK), BF16),
            pltpu.VMEM((2, 2 * ret_out.shape[0], n_fs // 2 * ret_out.shape[1]), BF16),
            pltpu.VMEM((n_sp,) + small, F32),
            pltpu.VMEM((DK, DV), F32),
            pltpu.VMEM((length, 3 * DK), BF16),
            pltpu.VMEM((WINDOW + length, 256), BF16),
            pltpu.VMEM((length, DV), BF16),
            pltpu.VMEM((2, n_sp, rows, DV), BF16),
            pltpu.VMEM((DK, DV), F32),
            pltpu.VMEM((rows, half), F32),
            dma((100,)),
            dma((n_sp, 3)),
            dma((n_sp, n_fs)),
            dma((n_sp,)),
            dma,
            dma,
            dma((n_sp, 2)),
            dma((2, 2, n_fs // 2)),
            dma((2, n_sp)),
            dma,
        ],
        compiler_params=pltpu.CompilerParams(
            collective_id=0, has_side_effects=True, vmem_limit_bytes=67043328
        ),
    )(
        tokens[0], norm_gain[None], ret_query, ret_key, ret_value, att_query, att_key, att_value,
        ret_gain[None], log_decay[0], sink_logits[None], start_state[0], ret_out, att_out, cos, sin,
    )
    return res[None]


def solution(mesh):
    placed = (
        P("fs", "sp", "tp"),
        P(),
        P("sp", "tp"),
        P("sp", "tp"),
        P("sp", "tp"),
        P("sp", "tp"),
        P("sp", "tp"),
        P("sp", "tp"),
        P("fs", "tp", "sp"),
        P("fs", "tp", None, None),
        P("tp"),
        P("tp"),
        P("tp", "fs"),
        P("tp", "fs"),
    )
    return jax.shard_map(
        functools.partial(layer, mesh), mesh=mesh, in_specs=placed, out_specs=P("fs", "sp", "tp"), check_vma=False
    )
```
